128 devices in a mesh: fs: 16 (over z, x), tp: 8 (over y, core).
Axes of the slice: x: 4, y: 4, z: 4, core: 2. Of those that a mesh axis runs over, the one named last changes fastest.
Arguments:
- stream: bfloat16 [8192, 2048], P('fs', 'tp'), may hold values from -6 to 6
- gain_mix: float32 [2048], replicated, may hold values from 0.1 to 1.9
- pool_weight: bfloat16 [4, 512, 512], P(None, 'fs', 'tp'), may hold values from -0.25 to 0.25
- pool_gain: float32 [2048], replicated, may hold values from 0.1 to 1.9
- gain_ffn: float32 [2048], replicated, may hold values from 0.1 to 1.9
- gate_weight: bfloat16 [2048, 5632], P('fs', 'tp'), may hold values from -0.125 to 0.125
- up_weight: bfloat16 [2048, 5632], P('fs', 'tp'), may hold values from -0.125 to 0.125
- gate_taps: float32 [3, 5632], replicated, may hold values from -2.5 to 2.5
- up_taps: float32 [3, 5632], replicated, may hold values from -2.5 to 2.5
- down_weight: bfloat16 [5632, 2048], P('tp', 'fs'), may hold values from -0.078125 to 0.078125
Outputs:
- layer_out: bfloat16 [8192, 2048], P('fs', 'tp')
The draws below stay inside these ranges and needn't reach their ends.
All inputs are finite; a program needn't handle non-finite values.
Results may differ from the reference program's by a relative error of at most 0.01.
Values may be sent and summed in bfloat16 or wider, within the bound.
A program may use at most 64 MiB of HBM per device.

```python
import jax
import jax.numpy as jnp
from jax import lax

D = 2048
G = 4
FF = 5632
TAPS = 3
LEN = 128
CG = 512
TOKENS = 8192


def level_of(own_key, dims, cuts, smallest, top_value):
    loudness, own = 1.0, jax.random.fold_in(own_key, 6)
    for axis_at, blocks in cuts:
        heights = jnp.exp(jax.random.uniform(jax.random.fold_in(own, axis_at), (blocks,), jnp.float32, smallest / len(cuts), top_value / len(cuts)))
        loudness = loudness * jnp.repeat(heights, dims[axis_at] // blocks).reshape([-1 if axis == axis_at else 1 for axis in range(len(dims))])
    return loudness


def scatter_about(own_key, shape, scale, limit, split=(), held_as=jnp.bfloat16):
    values = scale * jax.random.normal(own_key, shape, jnp.float32)
    if split:
        values = values * level_of(own_key, shape, split, -0.22, 0.18)
    return jnp.clip(values, -limit, limit).astype(held_as)


def setup_inputs(seed: int = 0) -> dict:
    streams_of = jax.random.split(jax.random.key(seed), 11)
    stream = scatter_about(streams_of[0], (TOKENS, D), 1.0, 6.0, ((0, 16), (1, 8)))
    gain_mix = jnp.clip(1.0 + 0.18 * jax.random.normal(streams_of[1], (D,), jnp.float32), 0.1, 1.9)
    pool_weight = scatter_about(streams_of[2], (G, CG, CG), CG ** -0.5, 0.25, ((1, 16), (2, 8)))
    pool_gain = jnp.clip(1.0 + 0.18 * jax.random.normal(streams_of[3], (D,), jnp.float32), 0.1, 1.9)
    gain_ffn = jnp.clip(1.0 + 0.18 * jax.random.normal(streams_of[4], (D,), jnp.float32), 0.1, 1.9)
    gate_weight = scatter_about(streams_of[5], (D, FF), D ** -0.5, 0.125, ((0, 16), (1, 8)))
    up_weight = scatter_about(streams_of[6], (D, FF), D ** -0.5, 0.125, ((0, 16), (1, 8)))
    gate_taps = scatter_about(streams_of[7], (TAPS, FF), 0.577, 2.5, (), jnp.float32)
    up_taps = scatter_about(streams_of[8], (TAPS, FF), 0.577, 2.5, (), jnp.float32)
    down_weight = scatter_about(streams_of[9], (FF, D), FF ** -0.5, 0.078125, ((0, 8), (1, 16)))
    return dict(stream=stream, gain_mix=gain_mix, pool_weight=pool_weight, pool_gain=pool_gain, gain_ffn=gain_ffn, gate_weight=gate_weight, up_weight=up_weight, gate_taps=gate_taps, up_taps=up_taps, down_weight=down_weight)


epsilon = 1e-06

def rms_norm(values, scales):
    return values * lax.rsqrt(lax.optimization_barrier(jnp.mean(values * values, axis=-1, keepdims=True)) + epsilon) * scales

def delayed(values, amount):
    return jnp.pad(values, ((0, 0), (amount, 0), (0, 0)))[:, :values.shape[1]]

def pool_less(values):
    channels = values.shape[2]
    group_id = jnp.arange(channels) % 4
    partials = [values]
    running = values
    for amount in (1, 2, 4, 8):
        running = running + delayed(running, amount)
        partials.append(running)
    picked = jnp.where(group_id == 0, partials[1], jnp.where(group_id == 1, partials[2], jnp.where(group_id == 2, partials[3], partials[4])))
    extent = jnp.where(group_id == 0, 2.0, jnp.where(group_id == 1, 4.0, jnp.where(group_id == 2, 8.0, 16.0)))
    position = jnp.arange(values.shape[1]).astype(jnp.float32)[:, None] + 1.0
    divisor = jnp.minimum(position, extent[None, :])
    return picked / divisor[None] - values

def causal_taps(values, kernel):
    reach = kernel.shape[0]
    length = values.shape[1]
    padded = jnp.pad(values, ((0, 0), (reach - 1, 0), (0, 0)))
    running = padded[:, 0:length] * kernel[0]
    for shift_by in range(1, reach):
        running = running + padded[:, shift_by:shift_by + length] * kernel[shift_by]
    return running

def reference(stream, gain_mix, pool_weight, pool_gain, gain_ffn, gate_weight, up_weight, gate_taps, up_taps, down_weight):
    tok_rows = stream.shape[0]
    seq_count = tok_rows // LEN
    normed = lax.optimization_barrier(rms_norm(stream.astype(jnp.float32), gain_mix).astype(jnp.bfloat16))
    pooled = pool_less(normed.astype(jnp.float32).reshape(seq_count, LEN, D)).astype(jnp.bfloat16)
    pooled = pooled.reshape(tok_rows, CG, G)
    mixer = jnp.einsum('tcg,gce->teg', pooled.astype(jnp.float32), pool_weight.astype(jnp.float32)).reshape(tok_rows, D) * pool_gain
    middle = lax.optimization_barrier((stream.astype(jnp.float32) + mixer).astype(jnp.bfloat16))
    normed_ffn = rms_norm(middle.astype(jnp.float32), gain_ffn).astype(jnp.bfloat16)
    gate_proj = lax.optimization_barrier(jnp.dot(normed_ffn, gate_weight, preferred_element_type=jnp.float32).astype(jnp.bfloat16))
    value_proj = lax.optimization_barrier(jnp.dot(normed_ffn, up_weight, preferred_element_type=jnp.float32).astype(jnp.bfloat16))
    gate_conv = causal_taps(gate_proj.astype(jnp.float32).reshape(seq_count, LEN, FF), gate_taps)
    value_conv = causal_taps(value_proj.astype(jnp.float32).reshape(seq_count, LEN, FF), up_taps)
    hidden = (jax.nn.silu(gate_conv) * value_conv).astype(jnp.bfloat16).reshape(tok_rows, FF)
    return jnp.dot(hidden, down_weight, preferred_element_type=jnp.float32).astype(jnp.bfloat16)
```

```python
import jax
import jax.numpy as jnp
from jax import lax
from jax.experimental import pallas as pl
from jax.experimental.pallas import tpu as pltpu
from jax.sharding import PartitionSpec as P

MESH = pl.DeviceIdType.MESH
bf16, f32 = jnp.bfloat16, jnp.float32
EPS = 1e-6
LEN = 128
TOK = 256


def concat(parts, axis):
    return jnp.concatenate(parts, axis=axis)


def iota(shape, dim):
    return lax.broadcasted_iota(jnp.int32, shape, dim)


def kernel(
    stream, gain_mix, pool_weight, pool_gain, gain_ffn, gate_weight, up_weight, gate_taps, up_taps,
    down_weight,
    out,
    gu, dn, pw, xs, sv, gwv, uwv, pv, gv, tv, taps, perm, unperm, band, gains, xg, wg, nf, acc, hid,
    pb, rbuf,
    lsem, gsem, dsem, psem, gd, dd, pys, pds, xys, xds, rsem, ssem,
):
    fs, tp = lax.axis_index("fs"), lax.axis_index("tp")
    z, x = fs // 4, fs % 4
    y, c = tp // 2, tp % 2

    def at_fs(dx, dz):
        return ((z + dz + 4) % 4) * 4 + (x + dx + 4) % 4

    def at_y(dy, core):
        return ((y + dy + 4) % 4) * 2 + core

    partner = (fs, y * 2 + (1 - c))

    barrier = pltpu.get_barrier_semaphore()
    peers = [(at_fs(1, 0), tp), (at_fs(-1, 0), tp), (at_fs(0, 1), tp), (at_fs(0, -1), tp)]
    peers += [(fs, (tp + d) % 8) for d in range(1, 8)]
    for peer in peers:
        pl.semaphore_signal(barrier, inc=1, device_id=peer, device_id_type=MESH)

    loads = [
        (gate_weight, gwv),
        (up_weight, uwv),
        (pool_weight, pv),
        (down_weight, dn.at[c, fs]),
        (stream.at[pl.ds(pl.multiple_of(c * TOK, TOK), TOK)], xs.at[y, c]),
        (stream.at[pl.ds(pl.multiple_of((1 - c) * TOK, TOK), TOK)], sv),
        (gain_mix, gv.at[0]),
        (pool_gain, gv.at[1]),
        (gain_ffn, gv.at[2]),
        (gate_taps.at[:, pl.ds(pl.multiple_of(y * 1408, 128), 1408)], tv.at[0]),
        (up_taps.at[:, pl.ds(pl.multiple_of(y * 1408, 128), 1408)], tv.at[1]),
    ]
    loads = [pltpu.make_async_copy(a, b, lsem.at[i]) for i, (a, b) in enumerate(loads)]
    for load in loads:
        load.start()
    for load in loads[:3]:
        load.wait()
    gu[c, fs, :, 0:640] = gwv[:, 0:640]
    gu[c, fs, :, 640:768] = concat([gwv[:, 640:704], uwv[:, 640:704]], 1)
    gu[c, fs, :, 768:1408] = uwv[:, 0:640]
    for p in range(2):
        pw[tp, fs, 32 * p : 32 * p + 32, :] = concat([pv[2 * p], pv[2 * p + 1]], 1)
    for load in loads[3:]:
        load.wait()
    pl.semaphore_wait(barrier, len(peers))

    def remote(src, dst, send, recv, device):
        return pltpu.make_async_remote_copy(
            src_ref=src, dst_ref=dst, send_sem=send, recv_sem=recv, device_id=device,
            device_id_type=MESH,
        )

    class Tree:
        def __init__(self, block, rows, recv, send):
            self.block, self.rows, self.recv, self.send = block, rows, recv, send

        def ref(self, q, a, b):
            color, sign = q // 2, 1 - 2 * (q % 2)
            j = at_fs(-sign * (a * (1 - color) + b * color), -sign * (a * color + b * (1 - color)))
            rows = pl.ds(pl.multiple_of(q * self.rows, self.rows), self.rows)
            return self.block(j).at[rows]

        def push(self, q, a, b, da, db):
            color, sign = q // 2, 1 - 2 * (q % 2)
            to = at_fs(sign * (da * (1 - color) + db * color), sign * (da * color + db * (1 - color)))
            ref = self.ref(q, a, b)
            pos = ((a + da) % 4) * 4 + (b + db) % 4
            remote(ref, ref, self.send, self.recv.at[q, pos], (to, tp)).start()

        def await_(self, q, a, b):
            ref = self.ref(q, a, b)
            pltpu.make_async_copy(ref, ref, self.recv.at[q, (a % 4) * 4 + b % 4]).wait()

        def each(self, f):
            def go(q, carry):
                f(q)
                return carry

            lax.fori_loop(0, 4, go, 0)

        def own(self):
            def f(q):
                self.push(q, 0, 0, 1, 0)
                self.push(q, 0, 0, -1, 0)
                self.push(q, 0, 0, 0, 1)
                self.push(q, 0, 0, 0, -1)

            self.each(f)

        def first(self):
            def f(q):
                self.await_(q, 1, 0)
                self.push(q, 1, 0, 1, 0)
                self.push(q, 1, 0, 0, 1)
                self.push(q, 1, 0, 0, -1)
                self.await_(q, -1, 0)
                self.push(q, -1, 0, 0, 1)
                self.push(q, -1, 0, 0, -1)

            self.each(f)

        def second(self):
            def f(q):
                self.await_(q, 2, 0)
                self.push(q, 2, 0, 0, 1)
                self.push(q, 2, 0, 0, -1)

            self.each(f)

        def cross(self, a):
            def f(q):
                self.await_(q, a, 1)
                self.push(q, a, 1, 0, 1)
                self.await_(q, a, -1)

            self.each(f)

        def end(self, a):
            self.each(lambda q: self.await_(q, a, 2))

    pool = Tree(lambda j: pw.at[tp, j], 16, psem, ssem.at[0])
    gup = Tree(lambda j: gu.at[c, j], 32, gsem, ssem.at[1])
    down = Tree(lambda j: dn.at[c, j], 176, dsem, ssem.at[2])

    def across(blocks, recv, send, offsets):
        for dx, dz in offsets:
            j, pos = at_fs(dx, dz), (dx % 4) * 4 + dz % 4
            remote(blocks.at[c, j], blocks.at[c, j], send, recv.at[pos], partner).start()

    def across_wait(blocks, recv, offsets):
        for dx, dz in offsets:
            j, pos = at_fs(dx, dz), (dx % 4) * 4 + dz % 4
            ref = blocks.at[1 - c, j]
            pltpu.make_async_copy(ref, ref, recv.at[pos]).wait()

    NEAR = [(1, 0), (-1, 0), (0, 1), (0, -1)]
    FAR = [(2, 0), (0, 2)]
    DIAG = [(1, 1), (1, -1), (-1, 1), (-1, -1)]
    KNIGHT = [(2, 1), (2, -1), (1, 2), (-1, 2)]
    ALL = [(0, 0)] + NEAR + FAR + DIAG + KNIGHT + [(2, 2)]

    def piece(dy, p):
        return xs.at[(y + dy + 4) % 4, p]

    def piece_out(p):
        remote(piece(0, p), piece(0, p), ssem.at[3], xys.at[p, 0], (fs, at_y(1, c))).start()
        remote(piece(0, p), piece(0, p), ssem.at[3], xys.at[p, 1], (fs, at_y(-1, c))).start()

    def got(ref, sem):
        pltpu.make_async_copy(ref, ref, sem).wait()

    remote(sv, xs.at[y, c], ssem.at[4], xds.at[0], partner).start()
    pool.own()
    piece_out(c)
    gup.own()
    across(gu, gd, ssem.at[5], [(0, 0)])
    across(dn, dd, ssem.at[6], [(0, 0)])

    d, n = iota((512, 512), 0), iota((512, 512), 1)
    perm[...] = ((d % 4) * 128 + d // 4 == n).astype(bf16)
    unperm[...] = ((n % 4) * 128 + n // 4 == d).astype(bf16)
    row, col = iota((LEN, LEN), 0), iota((LEN, LEN), 1)
    for g in range(4):
        band[g] = ((col <= row) & (col > row - 2 ** (g + 1))).astype(bf16)

    got(xs.at[y, 1 - c], xds.at[0])
    piece_out(1 - c)
    pool.first()
    pool.second()
    gup.first()

    three = concat([gv[0], gv[1], gv[2], jnp.zeros((5, 2048), f32)], 0)
    high = three.astype(bf16)
    rest = three - high.astype(f32)
    mid = rest.astype(bf16)
    low = (rest - mid.astype(f32)).astype(bf16)
    for yy in range(4):
        s = slice(512 * yy, 512 * yy + 512)
        moved = sum(jnp.dot(v[:, s], perm[...], preferred_element_type=f32) for v in (low, mid, high))
        for g in range(4):
            gains[g, :, 128 * yy : 128 * yy + 128] = moved[:, 128 * g : 128 * g + 128]
    for core in range(2):
        a = 704 * core
        gt, ut = tv[0, :, a : a + 704], tv[1, :, a : a + 704]
        taps[core, :, 0:640] = gt[:, 0:640]
        taps[core, :, 640:768] = concat([gt[:, 640:704], ut[:, 640:704]], 1)
        taps[core, :, 768:1408] = ut[:, 0:640]

    pool.cross(0)
    gup.second()
    pool.cross(1)
    pool.cross(-1)
    pool.cross(2)
    gup.cross(0)
    across(gu, gd, ssem.at[5], NEAR)
    for a in (0, 1, -1, 2):
        pool.end(a)

    def columns(dy, core):
        return pw.at[at_y(dy, core)]

    def pool_across(i, dy):
        remote(columns(dy, c), columns(dy, c), ssem.at[7], pds.at[i], partner).start()

    remote(columns(0, c), columns(0, c), ssem.at[8], pys.at[0], (fs, at_y(1, c))).start()
    remote(columns(0, c), columns(0, c), ssem.at[8], pys.at[1], (fs, at_y(-1, c))).start()
    pool_across(0, 0)

    got(piece(-1, 0), xys.at[0, 0])
    remote(piece(-1, 0), piece(-1, 0), ssem.at[3], xys.at[0, 2], (fs, at_y(1, c))).start()
    got(piece(1, 1), xys.at[1, 1])
    remote(piece(1, 1), piece(1, 1), ssem.at[3], xys.at[1, 2], (fs, at_y(-1, c))).start()
    got(piece(1, 0), xys.at[0, 1])
    got(piece(-1, 1), xys.at[1, 0])

    acc[...] = jnp.zeros_like(acc)

    def regroup(yy, carry):
        xp = jnp.dot(concat([xs[yy, 0], xs[yy, 1]], 1), perm[...], preferred_element_type=f32)
        at = pl.ds(pl.multiple_of(yy * 128, 128), 128)
        total = acc[...]
        for g in range(4):
            part = xp[:, 128 * g : 128 * g + 128]
            xg[g, :, at] = part.astype(bf16)
            total = total + part * part
        acc[...] = total
        return carry

    regroup(y, 0)
    gup.cross(1)
    regroup((y + 1) % 4, 0)
    gup.cross(-1)
    regroup((y + 3) % 4, 0)
    across(gu, gd, ssem.at[5], DIAG)
    gup.end(0)
    across(gu, gd, ssem.at[5], FAR)
    gup.cross(2)
    down.own()
    got(piece(2, 0), xys.at[0, 2])
    got(piece(2, 1), xys.at[1, 2])
    regroup((y + 2) % 4, 0)

    got(columns(-1, c), pys.at[0])
    half = columns(-1, c).at[0:8]
    remote(half, half, ssem.at[8], pys.at[2], (fs, at_y(1, c))).start()
    pool_across(1, -1)
    got(columns(1, c), pys.at[1])
    half = columns(1, c).at[8:16]
    remote(half, half, ssem.at[8], pys.at[3], (fs, at_y(-1, c))).start()
    pool_across(2, 1)

    def unpack(yy, carry):
        at = pl.ds(pl.multiple_of(yy * 128, 128), 128)
        for p in range(2):
            left = pw[2 * yy, :, 32 * p : 32 * p + 32, :].reshape(512, 128)
            right = pw[2 * yy + 1, :, 32 * p : 32 * p + 32, :].reshape(512, 128)
            wg[2 * p, :, at] = concat([left[:, 0:64], right[:, 0:64]], 1)
            wg[2 * p + 1, :, at] = concat([left[:, 64:128], right[:, 64:128]], 1)
        return carry

    got(columns(0, 1 - c), pds.at[0])
    unpack(y, 0)
    gup.end(1)
    gup.end(-1)
    got(columns(2, c).at[0:8], pys.at[2])
    got(columns(2, c).at[8:16], pys.at[3])
    pool_across(3, 2)
    got(columns(-1, 1 - c), pds.at[1])
    unpack((y + 3) % 4, 0)
    got(columns(1, 1 - c), pds.at[2])
    unpack((y + 1) % 4, 0)
    across(gu, gd, ssem.at[5], KNIGHT)
    gup.end(2)
    across(gu, gd, ssem.at[5], [(2, 2)])
    got(columns(2, 1 - c), pds.at[3])
    unpack((y + 2) % 4, 0)

    scale = lax.rsqrt(jnp.sum(acc[...], axis=1, keepdims=True) * (1.0 / 2048) + EPS)
    acc[...] = jnp.zeros_like(acc)
    position = iota((LEN, 512), 0) + 1

    def mix(g, carry):
        divisor = jnp.minimum(position, lax.shift_left(2, g)).astype(f32)
        normed = (xg[g].astype(f32) * scale * gains[g, 0:1, :]).astype(bf16)
        pooled = []
        for s in range(TOK // LEN):
            part = normed[LEN * s : LEN * s + LEN]
            window = jnp.dot(band[g], part, preferred_element_type=f32)
            pooled.append((window / divisor - part.astype(f32)).astype(bf16))
        mixer = jnp.dot(concat(pooled, 0), wg[g], preferred_element_type=f32) * gains[g, 1:2, :]
        middle = (xg[g].astype(f32) + mixer).astype(bf16)
        xg[g] = middle
        total = acc[...]
        for i in range(4):
            part = middle[:, 128 * i : 128 * i + 128].astype(f32)
            total = total + part * part
        acc[...] = total
        return carry

    lax.fori_loop(0, 4, mix, 0)
    down.first()
    scale = lax.rsqrt(jnp.sum(acc[...], axis=1, keepdims=True) * (1.0 / 2048) + EPS)

    def rescale(g, carry):
        xg[g] = (xg[g].astype(f32) * scale * gains[g, 2:3, :]).astype(bf16)
        return carry

    lax.fori_loop(0, 4, rescale, 0)

    def natural(yy, carry):
        at = pl.ds(pl.multiple_of(yy * 128, 128), 128)
        grouped = concat([xg[g, :, at] for g in range(4)], 1)
        moved = jnp.dot(grouped, unperm[...], preferred_element_type=f32).astype(bf16)
        nf[:, pl.ds(pl.multiple_of(yy * 512, 512), 512)] = moved
        return carry

    lax.fori_loop(0, 4, natural, 0)
    down.second()

    place = iota((TOK, 128), 0) % LEN

    def conv(core, at, width):
        block = gu[core, :, :, at : at + width].reshape(2048, width)
        v = jnp.dot(nf[...], block, preferred_element_type=f32).astype(bf16).astype(f32)
        outs = []
        for i in range(width // 128):
            part = v[:, 128 * i : 128 * i + 128]
            k = taps[core, :, at + 128 * i : at + 128 * i + 128]
            back1 = jnp.where(place >= 1, pltpu.roll(part, 1, 0), 0.0)
            back2 = jnp.where(place >= 2, pltpu.roll(part, 2, 0), 0.0)
            outs.append(back2 * k[0:1] + back1 * k[1:2] + part * k[2:3])
        return outs

    def gated(a, b):
        return (a / (1.0 + jnp.exp(-a)) * b).astype(bf16)

    def units(core, t):
        for i, (a, b) in enumerate(zip(conv(core, 256 * t, 256), conv(core, 768 + 256 * t, 256))):
            at = 256 * t + 128 * i
            hid[core, :, at : at + 128] = gated(a, b)

    def last_units(core):
        a, both = conv(core, 512, 256)
        (b,) = conv(core, 1280, 128)
        hid[core, :, 512:640] = gated(a, b)
        hid[core, :, 640:704] = gated(both[:, 0:64], both[:, 64:128])

    units(c, 0)
    down.cross(0)
    across(dn, dd, ssem.at[6], NEAR)
    units(c, 1)
    down.end(0)
    across(dn, dd, ssem.at[6], FAR)
    last_units(c)
    down.cross(1)
    down.cross(-1)
    across(dn, dd, ssem.at[6], DIAG)
    across_wait(gu, gd, ALL)
    units(1 - c, 0)
    down.cross(2)
    units(1 - c, 1)
    last_units(1 - c)

    def owner_columns(dz, other):
        xpair = x // 2 if other == 0 else 1 - x // 2
        zk = (z + dz + 4) % 4
        k = zk * 2 + xpair
        total = None
        for core in range(2):
            block = concat([dn[core, 2 * k], dn[core, 2 * k + 1]], 1)
            part = jnp.dot(hid[core], block, preferred_element_type=f32)
            total = part if total is None else total + part
        pb[k] = total.astype(bf16)
        own = k == tp

        @pl.when(own)
        def _():
            rbuf[tp] = total.astype(bf16)

        @pl.when(jnp.logical_not(own))
        def _():
            remote(pb.at[k], rbuf.at[tp], ssem.at[9], rsem.at[tp], (fs, k)).start()

    down.end(1)
    down.end(-1)
    across(dn, dd, ssem.at[6], KNIGHT)
    down.end(2)
    across(dn, dd, ssem.at[6], [(2, 2)])
    across_wait(dn, dd, ALL)
    for dz in (0, 1, -1, 2):
        for other in (0, 1):
            owner_columns(dz, other)

    for i in range(1, 8):
        src = (tp + i) % 8
        got(rbuf.at[src], rsem.at[src])
    for core in range(2):
        total = rbuf[core].astype(f32)
        for yy in range(1, 4):
            total = total + rbuf[2 * yy + core].astype(f32)
        out[TOK * core : TOK * core + TOK, :] = total.astype(bf16)

    for ref, i in (
        (pw.at[0, 0:15], 0), (gu.at[0, 0:15], 1), (dn.at[0, 0:15], 2), (xs.at[0:3], 3), (sv, 4),
        (gu.at[0], 5), (dn.at[0], 6), (pw.at[0:4], 7), (pw.at[0:3], 8), (pb.at[0:7], 9),
    ):
        got(ref, ssem.at[i])


def body(
    stream, gain_mix, pool_weight, pool_gain, gain_ffn, gate_weight, up_weight, gate_taps, up_taps,
    down_weight,
):
    row = lambda v: v.reshape(1, 2048)
    DMA = pltpu.SemaphoreType.DMA
    return pl.pallas_call(
        kernel,
        name="layer",
        out_shape=jax.ShapeDtypeStruct((512, 256), bf16),
        in_specs=[pl.BlockSpec(memory_space=pl.ANY)] * 10,
        out_specs=pl.BlockSpec(memory_space=pltpu.VMEM),
        scratch_shapes=[
            pltpu.VMEM((2, 16, 128, 1408), bf16),
            pltpu.VMEM((2, 16, 704, 128), bf16),
            pltpu.VMEM((8, 16, 64, 128), bf16),
            pltpu.VMEM((4, 2, TOK, 256), bf16),
            pltpu.VMEM((TOK, 256), bf16),
            pltpu.VMEM((128, 704), bf16),
            pltpu.VMEM((128, 704), bf16),
            pltpu.VMEM((4, 32, 64), bf16),
            pltpu.VMEM((3, 1, 2048), f32),
            pltpu.VMEM((2, 3, 1408), f32),
            pltpu.VMEM((2, 3, 1408), f32),
            pltpu.VMEM((512, 512), bf16),
            pltpu.VMEM((512, 512), bf16),
            pltpu.VMEM((4, LEN, LEN), bf16),
            pltpu.VMEM((4, 8, 512), f32),
            pltpu.VMEM((4, TOK, 512), bf16),
            pltpu.VMEM((4, 512, 512), bf16),
            pltpu.VMEM((TOK, 2048), bf16),
            pltpu.VMEM((TOK, 128), f32),
            pltpu.VMEM((2, TOK, 704), bf16),
            pltpu.VMEM((8, TOK, 256), bf16),
            pltpu.VMEM((8, TOK, 256), bf16),
            DMA((11,)),
            DMA((4, 16)),
            DMA((4, 16)),
            DMA((4, 16)),
            DMA((16,)),
            DMA((16,)),
            DMA((4,)),
            DMA((4,)),
            DMA((2, 3)),
            DMA((1,)),
            DMA((8,)),
            DMA((10,)),
        ],
        compiler_params=pltpu.CompilerParams(
            collective_id=0, has_side_effects=True, vmem_limit_bytes=60 * 1024 * 1024
        ),
    )(
        stream, row(gain_mix), pool_weight, row(pool_gain), row(gain_ffn), gate_weight, up_weight,
        gate_taps, up_taps, down_weight,
    )


def solution(mesh):
    return jax.shard_map(
        body,
        mesh=mesh,
        in_specs=(
            P("fs", "tp"), P(), P(None, "fs", "tp"), P(), P(), P("fs", "tp"), P("fs", "tp"), P(), P(),
            P("tp", "fs"),
        ),
        out_specs=P("fs", "tp"),
        check_vma=False,
    )
```

```python
import jax
import jax.numpy as jnp
from jax import lax
from jax.experimental import pallas as pl
from jax.experimental.pallas import tpu as pltpu
from jax.sharding import PartitionSpec as P

MESH = pl.DeviceIdType.MESH
bf16, f32 = jnp.bfloat16, jnp.float32
EPS = 1e-6
LEN = 128
TOK = 256


def concat(parts, axis):
    return jnp.concatenate(parts, axis=axis)


def iota(shape, dim):
    return lax.broadcasted_iota(jnp.int32, shape, dim)


def kernel(
    stream, gain_mix, pool_weight, pool_gain, gain_ffn, gate_weight, up_weight, gate_taps, up_taps,
    down_weight,
    out,
    gu, dn, pw, xs, sv, pv, gv, tv, taps, perm, unperm, band, gains, xg, wg, nf, acc, hid,
    pb, rbuf, sums, relay_in,
    lsem, gsem, dsem, psem, gd, dd, pys, pds, xys, xds, rsem, ssem, relsem,
):
    fs, tp = lax.axis_index("fs"), lax.axis_index("tp")
    z, x = fs // 4, fs % 4
    y, c = tp // 2, tp % 2

    def at_fs(dx, dz):
        return ((z + dz + 4) % 4) * 4 + (x + dx + 4) % 4

    def at_y(dy, core):
        return ((y + dy + 4) % 4) * 2 + core

    partner = (fs, y * 2 + (1 - c))

    barrier = pltpu.get_barrier_semaphore()
    others = [(dx, dz) for dz in (0, 1, -1, 2) for dx in (0, 1, -1, 2)][1:]
    peers = [(at_fs(dx, dz), tp) for dx, dz in others]
    peers += [(fs, at_y(dy, core)) for dy in (1, -1) for core in (0, 1)] + [partner]
    for peer in peers:
        pl.semaphore_signal(barrier, inc=1, device_id=peer, device_id_type=MESH)

    loads = [
        (pool_weight, pv),
        (gate_weight, gu.at[c, fs, pl.ds(0, 704)]),
        (up_weight, gu.at[c, fs, pl.ds(704, 704)]),
        (down_weight, dn.at[c, fs]),
        (stream.at[pl.ds(pl.multiple_of(c * TOK, TOK), TOK)], xs.at[y, c]),
        (stream.at[pl.ds(pl.multiple_of((1 - c) * TOK, TOK), TOK)], sv),
        (gain_mix, gv.at[0]),
        (pool_gain, gv.at[1]),
        (gain_ffn, gv.at[2]),
        (gate_taps.at[:, pl.ds(pl.multiple_of(y * 1408, 128), 1408)], tv.at[0]),
        (up_taps.at[:, pl.ds(pl.multiple_of(y * 1408, 128), 1408)], tv.at[1]),
    ]
    loads = [pltpu.make_async_copy(a, b, lsem.at[i]) for i, (a, b) in enumerate(loads)]
    for load in loads:
        load.start()
    loads[0].wait()
    for p in range(2):
        pw[tp, fs, 32 * p : 32 * p + 32, :] = concat([pv[2 * p], pv[2 * p + 1]], 1)
    for load in loads[1:]:
        load.wait()
    pl.semaphore_wait(barrier, len(peers))

    def remote(src, dst, send, recv, device):
        return pltpu.make_async_remote_copy(
            src_ref=src, dst_ref=dst, send_sem=send, recv_sem=recv, device_id=device,
            device_id_type=MESH,
        )

    class Tree:
        def __init__(self, block, rows, recv, send):
            self.block, self.rows, self.recv, self.send = block, rows, recv, send

        def ref(self, q, a, b):
            color, sign = q // 2, 1 - 2 * (q % 2)
            j = at_fs(-sign * (a * (1 - color) + b * color), -sign * (a * color + b * (1 - color)))
            rows = pl.ds(pl.multiple_of(q * self.rows, self.rows), self.rows)
            return self.block(j).at[rows]

        def push(self, q, a, b, da, db):
            color, sign = q // 2, 1 - 2 * (q % 2)
            to = at_fs(sign * (da * (1 - color) + db * color), sign * (da * color + db * (1 - color)))
            ref = self.ref(q, a, b)
            pos = ((a + da) % 4) * 4 + (b + db) % 4
            remote(ref, ref, self.send, self.recv.at[pos], (to, tp)).start()

        def await_(self, a, b):
            ref = self.block(fs)
            pltpu.make_async_copy(ref, ref, self.recv.at[(a % 4) * 4 + b % 4]).wait()

        def each(self, f):
            def go(q, carry):
                f(q)
                return carry

            lax.fori_loop(0, 4, go, 0)

        def run(self, *items):
            for a, b, wait, steps in items:
                if wait:
                    self.await_(a, b)

                def f(q):
                    for da, db in steps:
                        self.push(q, a, b, da, db)

                if steps:
                    self.each(f)

    gup = Tree(lambda j: gu.at[c, j], 352, gsem, ssem.at[1])
    down = Tree(lambda j: dn.at[c, j], 176, dsem, ssem.at[2])

    def across(blocks, recv, send, offsets):
        for dx, dz in offsets:
            j, pos = at_fs(dx, dz), (dx % 4) * 4 + dz % 4
            remote(blocks.at[c, j], blocks.at[c, j], send, recv.at[pos], partner).start()

    def across_wait(blocks, recv, offsets):
        for dx, dz in offsets:
            j, pos = at_fs(dx, dz), (dx % 4) * 4 + dz % 4
            ref = blocks.at[1 - c, j]
            pltpu.make_async_copy(ref, ref, recv.at[pos]).wait()

    NEAR = [(1, 0), (-1, 0), (0, 1), (0, -1)]
    FAR = [(2, 0), (0, 2)]
    DIAG = [(1, 1), (1, -1), (-1, 1), (-1, -1)]
    KNIGHT = [(2, 1), (2, -1), (1, 2), (-1, 2)]
    ALL = [(0, 0)] + NEAR + FAR + DIAG + KNIGHT + [(2, 2)]

    def piece(dy, p):
        return xs.at[(y + dy + 4) % 4, p]

    def piece_out(p):
        remote(piece(0, p), piece(0, p), ssem.at[3], xys.at[p, 0], (fs, at_y(1, c))).start()
        remote(piece(0, p), piece(0, p), ssem.at[3], xys.at[p, 1], (fs, at_y(-1, c))).start()

    def got(ref, sem):
        pltpu.make_async_copy(ref, ref, sem).wait()

    RIGHT, LEFT, UP, DOWN = (1, 0), (-1, 0), (0, 1), (0, -1)
    remote(sv, xs.at[y, c], ssem.at[4], xds.at[0], partner).start()
    piece_out(c)
    for dx, dz in others:
        mine = pw.at[tp, fs]
        remote(mine, mine, ssem.at[0], psem.at[0], (at_fs(dx, dz), tp)).start()
    gup.run((0, 0, False, [RIGHT]))
    gup.run((0, 0, False, [UP]))
    gup.run((0, 0, False, [LEFT]))
    across(gu, gd, ssem.at[5], [(0, 0)])
    across(dn, dd, ssem.at[6], [(0, 0)])

    d, n = iota((512, 512), 0), iota((512, 512), 1)
    perm[...] = ((d % 4) * 128 + d // 4 == n).astype(bf16)
    unperm[...] = ((n % 4) * 128 + n // 4 == d).astype(bf16)
    row, col = iota((LEN, LEN), 0), iota((LEN, LEN), 1)
    for g in range(4):
        band[g] = ((col <= row) & (col > row - 2 ** (g + 1))).astype(bf16)

    got(xs.at[y, 1 - c], xds.at[0])
    piece_out(1 - c)

    three = concat([gv[0], gv[1], gv[2], jnp.zeros((5, 2048), f32)], 0)
    high = three.astype(bf16)
    rest = three - high.astype(f32)
    mid = rest.astype(bf16)
    low = (rest - mid.astype(f32)).astype(bf16)
    for yy in range(4):
        s = slice(512 * yy, 512 * yy + 512)
        moved = sum(jnp.dot(v[:, s], perm[...], preferred_element_type=f32) for v in (low, mid, high))
        for g in range(4):
            gains[g, :, 128 * yy : 128 * yy + 128] = moved[:, 128 * g : 128 * g + 128]
    for core in range(2):
        a = 704 * core
        taps[core, 0] = tv[0, :, a : a + 704]
        taps[core, 1] = tv[1, :, a : a + 704]

    gup.run((1, 0, True, [RIGHT]))
    gup.run((0, 0, False, [DOWN]))
    gup.run((1, 0, False, [UP]))
    got(pw.at[tp, 0:15], psem.at[0])

    def columns(dy, core):
        return pw.at[at_y(dy, core)]

    def pool_across(i, dy):
        remote(columns(dy, c), columns(dy, c), ssem.at[7], pds.at[i], partner).start()

    remote(columns(0, c), columns(0, c), ssem.at[8], pys.at[0], (fs, at_y(1, c))).start()
    remote(columns(0, c), columns(0, c), ssem.at[8], pys.at[1], (fs, at_y(-1, c))).start()
    pool_across(0, 0)
    gup.run((2, 0, True, [UP]))

    got(piece(-1, 0), xys.at[0, 0])
    remote(piece(-1, 0), piece(-1, 0), ssem.at[3], xys.at[0, 2], (fs, at_y(1, c))).start()
    got(piece(1, 1), xys.at[1, 1])
    remote(piece(1, 1), piece(1, 1), ssem.at[3], xys.at[1, 2], (fs, at_y(-1, c))).start()
    gup.run((-1, 0, True, [UP]))
    gup.run((0, 1, True, [UP]), (1, 0, False, [DOWN]), (2, 0, False, [DOWN]), (-1, 0, False, [DOWN]))

    acc[...] = jnp.zeros_like(acc)

    def regroup(yy, carry):
        xp = jnp.dot(concat([xs[yy, 0], xs[yy, 1]], 1), perm[...], preferred_element_type=f32)
        at = pl.ds(pl.multiple_of(yy * 128, 128), 128)
        total = acc[...]
        for g in range(4):
            part = xp[:, 128 * g : 128 * g + 128]
            xg[g, :, at] = part.astype(bf16)
            total = total + part * part
        acc[...] = total
        return carry

    def unpack(yy, carry):
        at = pl.ds(pl.multiple_of(yy * 128, 128), 128)
        for p in range(2):
            left = pw[2 * yy, :, 32 * p : 32 * p + 32, :].reshape(512, 128)
            right = pw[2 * yy + 1, :, 32 * p : 32 * p + 32, :].reshape(512, 128)
            wg[2 * p, :, at] = concat([left[:, 0:64], right[:, 0:64]], 1)
            wg[2 * p + 1, :, at] = concat([left[:, 64:128], right[:, 64:128]], 1)
        return carry

    got(piece(1, 0), xys.at[0, 1])
    got(piece(-1, 1), xys.at[1, 0])
    regroup(y, 0)
    gup.run((0, -1, True, []))
    across(gu, gd, ssem.at[5], NEAR)
    regroup((y + 1) % 4, 0)
    regroup((y + 3) % 4, 0)
    got(columns(0, 1 - c), pds.at[0])
    unpack(y, 0)
    got(columns(-1, c), pys.at[0])
    half = columns(-1, c).at[0:8]
    remote(half, half, ssem.at[8], pys.at[2], (fs, at_y(1, c))).start()
    pool_across(1, -1)
    got(columns(1, c), pys.at[1])
    half = columns(1, c).at[8:16]
    remote(half, half, ssem.at[8], pys.at[3], (fs, at_y(-1, c))).start()
    pool_across(2, 1)
    gup.run((1, 1, True, [UP]))
    down.run((0, 0, False, [RIGHT]))
    gup.run((2, 1, True, [UP]))
    down.run((0, 0, False, [UP]))
    gup.run((-1, 1, True, [UP]))
    down.run((0, 0, False, [LEFT]))
    down.run((0, 0, False, [DOWN]))
    got(piece(2, 0), xys.at[0, 2])
    got(piece(2, 1), xys.at[1, 2])
    regroup((y + 2) % 4, 0)
    got(columns(-1, 1 - c), pds.at[1])
    unpack((y + 3) % 4, 0)
    got(columns(1, 1 - c), pds.at[2])
    unpack((y + 1) % 4, 0)
    got(columns(2, c).at[0:8], pys.at[2])
    got(columns(2, c).at[8:16], pys.at[3])
    pool_across(3, 2)
    got(columns(2, 1 - c), pds.at[3])
    unpack((y + 2) % 4, 0)
    gup.run((0, 2, True, []))
    across(gu, gd, ssem.at[5], FAR)

    scale = lax.rsqrt(jnp.sum(acc[...], axis=1, keepdims=True) * (1.0 / 2048) + EPS)
    acc[...] = jnp.zeros_like(acc)
    position = iota((LEN, 512), 0) + 1

    def mix(g, carry):
        divisor = jnp.minimum(position, lax.shift_left(2, g)).astype(f32)
        normed = (xg[g].astype(f32) * scale * gains[g, 0:1, :]).astype(bf16)
        pooled = []
        for s in range(TOK // LEN):
            part = normed[LEN * s : LEN * s + LEN]
            window = jnp.dot(band[g], part, preferred_element_type=f32)
            pooled.append((window / divisor - part.astype(f32)).astype(bf16))
        mixer = jnp.dot(concat(pooled, 0), wg[g], preferred_element_type=f32) * gains[g, 1:2, :]
        middle = (xg[g].astype(f32) + mixer).astype(bf16)
        xg[g] = middle
        total = acc[...]
        for i in range(4):
            part = middle[:, 128 * i : 128 * i + 128].astype(f32)
            total = total + part * part
        acc[...] = total
        return carry

    lax.fori_loop(0, 4, mix, 0)
    scale = lax.rsqrt(jnp.sum(acc[...], axis=1, keepdims=True) * (1.0 / 2048) + EPS)

    def rescale(g, carry):
        xg[g] = (xg[g].astype(f32) * scale * gains[g, 2:3, :]).astype(bf16)
        return carry

    lax.fori_loop(0, 4, rescale, 0)

    def natural(yy, carry):
        at = pl.ds(pl.multiple_of(yy * 128, 128), 128)
        grouped = concat([xg[g, :, at] for g in range(4)], 1)
        moved = jnp.dot(grouped, unperm[...], preferred_element_type=f32).astype(bf16)
        for i in range(4):
            nf[4 * yy + i] = moved[:, 128 * i : 128 * i + 128]
        return carry

    lax.fori_loop(0, 4, natural, 0)

    SETS = ([(0, 0)] + NEAR, FAR + DIAG, KNIGHT + [(2, 2)])
    CHUNKS = ((0, 256), (256, 256), (512, 192))

    def product(core, which, at, width, offsets):
        js = [at_fs(dx, dz) for dx, dz in offsets]
        left = concat([nf[j] for j in js], 1)
        right = concat([gu[core, j, pl.ds(704 * which + at, width), :] for j in js], 1)
        return lax.dot_general(left, right, (((1,), (1,)), ((), ())), preferred_element_type=f32)

    def gather_up(core, i):
        for which in range(2):
            for at, width in CHUNKS:
                part = product(core, which, at, width, SETS[i])
                if i > 0:
                    part = sums[core, which, :, at : at + width] + part
                sums[core, which, :, at : at + width] = part

    def conv(core, which, at, width):
        v = sums[core, which, :, at : at + width] + product(core, which, at, width, SETS[2])
        v = v.astype(bf16).astype(f32)
        k = taps[core, which, :, at : at + width]
        place = iota((TOK, width), 0) % LEN
        back1 = jnp.where(place >= 1, pltpu.roll(v, 1, 0), 0.0)
        back2 = jnp.where(place >= 2, pltpu.roll(v, 2, 0), 0.0)
        return back2 * k[0:1] + back1 * k[1:2] + v * k[2:3]

    def units(core, t):
        at, width = CHUNKS[t]
        a, b = conv(core, 0, at, width), conv(core, 1, at, width)
        hid[core, :, at : at + width] = (a / (1.0 + jnp.exp(-a)) * b).astype(bf16)

    gather_up(c, 0)
    across_wait(gu, gd, SETS[0])
    gather_up(1 - c, 0)
    gup.run((1, -1, True, []), (-1, -1, True, []), (2, -1, True, []))
    across(gu, gd, ssem.at[5], DIAG)
    gather_up(c, 1)
    across_wait(gu, gd, SETS[1])
    gather_up(1 - c, 1)
    down.run((1, 0, True, [RIGHT, UP]))
    gup.run((1, 2, True, []), (2, 2, True, []))
    down.run((0, 1, True, [UP]))
    gup.run((-1, 2, True, []))
    across(gu, gd, ssem.at[5], KNIGHT + [(2, 2)])
    units(c, 0)
    down.run((-1, 0, True, [UP, DOWN]), (1, 0, False, [DOWN]))
    units(c, 1)
    down.run((0, -1, True, []))
    across(dn, dd, ssem.at[6], NEAR)
    units(c, 2)
    down.run((2, 0, True, [UP, DOWN]))
    across_wait(gu, gd, SETS[2])
    units(1 - c, 0)
    down.run((1, 1, True, [UP]))
    units(1 - c, 1)
    down.run((-1, 1, True, [UP]))
    units(1 - c, 2)

    way = {(0, 0): 1, (0, 1): -1, (1, 0): -1, (1, 1): 1, (-1, 0): 1, (-1, 1): -1, (2, 0): 1, (2, 1): -1}

    def pair_of(dz, other):
        cols = x // 2 if other == 0 else 1 - x // 2
        zk = (z + dz + 4) % 4
        return zk * 2 + cols, cols, (zk - y + 4) % 4

    def to_owner(k, dy, cols):
        slot = 1 if dy == 1 else 2
        device = (fs, at_y(dy, cols))
        remote(pb.at[k], rbuf.at[slot, c], ssem.at[9], rsem.at[slot, c], device).start()

    def owner_columns(dz, other):
        k, cols, role = pair_of(dz, other)
        dy = way[dz, other]
        total = None
        for core in range(2):
            block = concat([dn[core, 2 * k], dn[core, 2 * k + 1]], 1)
            part = jnp.dot(hid[core], block, preferred_element_type=f32)
            total = part if total is None else total + part
        pb[k] = total.astype(bf16)

        @pl.when((role == 0) & (cols == c))
        def _():
            rbuf[0, c] = pb[k]

        @pl.when((role == 0) & (cols != c))
        def _():
            remote(pb.at[k], rbuf.at[0, c], ssem.at[9], rsem.at[0, c], partner).start()

        @pl.when(role == (3 if dy == 1 else 1))
        def _():
            to_owner(k, -dy, cols)

        @pl.when(role == 2)
        def _():
            slot = (1 - dy) // 2
            device = (fs, at_y(dy, c))
            remote(pb.at[k], relay_in.at[slot], ssem.at[9], relsem.at[slot], device).start()

    def owner_added(dz, other):
        k, cols, role = pair_of(dz, other)
        dy = way[dz, other]
        slot = (1 - dy) // 2

        @pl.when(role == (1 if dy == 1 else 3))
        def _():
            got(relay_in.at[slot], relsem.at[slot])
            pb[k] = (pb[k].astype(f32) + relay_in[slot].astype(f32)).astype(bf16)
            to_owner(k, dy, cols)

    across_wait(dn, dd, [(0, 0)] + NEAR)
    owner_columns(0, 0)
    down.run((0, 2, True, []))
    across(dn, dd, ssem.at[6], FAR)
    down.run((1, -1, True, []), (-1, -1, True, []), (2, -1, True, []))
    across(dn, dd, ssem.at[6], DIAG)
    across_wait(dn, dd, FAR)
    owner_columns(0, 1)
    down.run((2, 1, True, [UP]))
    owner_added(0, 0)
    down.run((1, 2, True, []), (-1, 2, True, []))
    across(dn, dd, ssem.at[6], KNIGHT)
    across_wait(dn, dd, DIAG)
    owner_columns(1, 0)
    owner_columns(-1, 0)
    down.run((2, 2, True, []))
    across(dn, dd, ssem.at[6], [(2, 2)])
    across_wait(dn, dd, KNIGHT)
    owner_columns(2, 0)
    owner_columns(1, 1)
    owner_added(0, 1)
    owner_columns(-1, 1)
    owner_added(1, 0)
    across_wait(dn, dd, [(2, 2)])
    owner_columns(2, 1)
    owner_added(-1, 0)
    owner_added(2, 0)
    owner_added(1, 1)
    owner_added(-1, 1)
    owner_added(2, 1)

    got(rbuf.at[1, 0], rsem.at[1, 0])
    got(rbuf.at[1, 1], rsem.at[1, 1])
    got(rbuf.at[2, 0], rsem.at[2, 0])
    got(rbuf.at[2, 1], rsem.at[2, 1])
    got(rbuf.at[0, 1 - c], rsem.at[0, 1 - c])
    for core in range(2):
        total = rbuf[0, core].astype(f32) + rbuf[1, core].astype(f32) + rbuf[2, core].astype(f32)
        out[TOK * core : TOK * core + TOK, :] = total.astype(bf16)

    for ref, i in (
        (pw.at[0, 0:15], 0), (gu.at[0, 0:15], 1), (dn.at[0, 0:15], 2), (xs.at[0:3], 3), (sv, 4),
        (gu.at[0], 5), (dn.at[0], 6), (pw.at[0:4], 7), (pw.at[0:3], 8), (pb.at[0:7], 9),
    ):
        got(ref, ssem.at[i])


def body(
    stream, gain_mix, pool_weight, pool_gain, gain_ffn, gate_weight, up_weight, gate_taps, up_taps,
    down_weight,
):
    row = lambda v: v.reshape(1, 2048)
    DMA = pltpu.SemaphoreType.DMA
    return pl.pallas_call(
        kernel,
        name="layer",
        out_shape=jax.ShapeDtypeStruct((512, 256), bf16),
        in_specs=[pl.BlockSpec(memory_space=pltpu.HBM)] * 10,
        out_specs=pl.BlockSpec(memory_space=pltpu.VMEM),
        scratch_shapes=[
            pltpu.VMEM((2, 16, 1408, 128), bf16),
            pltpu.VMEM((2, 16, 704, 128), bf16),
            pltpu.VMEM((8, 16, 64, 128), bf16),
            pltpu.VMEM((4, 2, TOK, 256), bf16),
            pltpu.VMEM((TOK, 256), bf16),
            pltpu.VMEM((4, 32, 64), bf16),
            pltpu.VMEM((3, 1, 2048), f32),
            pltpu.VMEM((2, 3, 1408), f32),
            pltpu.VMEM((2, 2, 3, 704), f32),
            pltpu.VMEM((512, 512), bf16),
            pltpu.VMEM((512, 512), bf16),
            pltpu.VMEM((4, LEN, LEN), bf16),
            pltpu.VMEM((4, 8, 512), f32),
            pltpu.VMEM((4, TOK, 512), bf16),
            pltpu.VMEM((4, 512, 512), bf16),
            pltpu.VMEM((16, TOK, 128), bf16),
            pltpu.VMEM((TOK, 128), f32),
            pltpu.VMEM((2, TOK, 704), bf16),
            pltpu.VMEM((8, TOK, 256), bf16),
            pltpu.VMEM((3, 2, TOK, 256), bf16),
            pltpu.VMEM((2, 2, TOK, 704), f32),
            pltpu.VMEM((2, TOK, 256), bf16),
            DMA((11,)),
            DMA((16,)),
            DMA((16,)),
            DMA((1,)),
            DMA((16,)),
            DMA((16,)),
            DMA((4,)),
            DMA((4,)),
            DMA((2, 3)),
            DMA((1,)),
            DMA((3, 2)),
            DMA((10,)),
            DMA((2,)),
        ],
        compiler_params=pltpu.CompilerParams(
            collective_id=0, has_side_effects=True, vmem_limit_bytes=60 * 1024 * 1024
        ),
    )(
        stream, row(gain_mix), pool_weight, row(pool_gain), row(gain_ffn), gate_weight.T, up_weight.T,
        gate_taps, up_taps, down_weight,
    )


def solution(mesh):
    return jax.shard_map(
        body,
        mesh=mesh,
        in_specs=(
            P("fs", "tp"), P(), P(None, "fs", "tp"), P(), P(), P("fs", "tp"), P("fs", "tp"), P(), P(),
            P("tp", "fs"),
        ),
        out_specs=P("fs", "tp"),
        check_vma=False,
    )
```

```python
import jax
import jax.numpy as jnp
from jax import lax
from jax.experimental import pallas as pl
from jax.experimental.pallas import tpu as pltpu
from jax.sharding import PartitionSpec as P

MESH = pl.DeviceIdType.MESH
bf16, f32 = jnp.bfloat16, jnp.float32
EPS = 1e-6
LEN = 128
TOK = 256


def concat(parts, axis):
    return jnp.concatenate(parts, axis=axis)


def iota(shape, dim):
    return lax.broadcasted_iota(jnp.int32, shape, dim)


def kernel(
    stream, gain_mix, pool_weight, pool_gain, gain_ffn, gate_weight, up_weight, gate_taps, up_taps,
    down_weight,
    out,
    gu, dn, pw, xs, sv, pv, gv, tv, taps, perm, unperm, band, gains, xg, wg, nf, acc, hid,
    pb, rbuf, sums, relay_in, early,
    lsem, gsem, dsem, psem, gd, dd, pys, pds, xys, xds, rsem, ssem, relsem,
):
    fs, tp = lax.axis_index("fs"), lax.axis_index("tp")
    z, x = fs // 4, fs % 4
    y, c = tp // 2, tp % 2

    def at_fs(dx, dz):
        return ((z + dz + 4) % 4) * 4 + (x + dx + 4) % 4

    def at_y(dy, core):
        return ((y + dy + 4) % 4) * 2 + core

    partner = (fs, y * 2 + (1 - c))

    barrier = pltpu.get_barrier_semaphore()
    near = [(dx, dz) for dz in (0, 1, -1) for dx in (0, 1, -1)][1:]
    peers = [(at_fs(dx, dz), tp) for dx, dz in near]
    peers += [(fs, at_y(dy, core)) for dy in (1, -1) for core in (0, 1)] + [partner]
    for peer in peers:
        pl.semaphore_signal(barrier, inc=1, device_id=peer, device_id_type=MESH)

    loads = [
        (pool_weight, pv),
        (gate_weight, gu.at[c, fs, pl.ds(0, 704)]),
        (up_weight, gu.at[c, fs, pl.ds(704, 704)]),
        (down_weight, dn.at[c, fs]),
        (stream.at[pl.ds(pl.multiple_of(c * TOK, TOK), TOK)], xs.at[y, c]),
        (stream.at[pl.ds(pl.multiple_of((1 - c) * TOK, TOK), TOK)], sv),
        (gain_mix, gv.at[0]),
        (pool_gain, gv.at[1]),
        (gain_ffn, gv.at[2]),
        (gate_taps.at[:, pl.ds(pl.multiple_of(y * 1408, 128), 1408)], tv.at[0]),
        (up_taps.at[:, pl.ds(pl.multiple_of(y * 1408, 128), 1408)], tv.at[1]),
    ]
    loads = [pltpu.make_async_copy(a, b, lsem.at[i]) for i, (a, b) in enumerate(loads)]
    for load in loads:
        load.start()
    loads[0].wait()
    for p in range(2):
        pw[tp, fs, 32 * p : 32 * p + 32, :] = concat([pv[2 * p], pv[2 * p + 1]], 1)
    for load in loads[1:]:
        load.wait()
    pl.semaphore_wait(barrier, len(peers))

    def remote(src, dst, send, recv, device):
        return pltpu.make_async_remote_copy(
            src_ref=src, dst_ref=dst, send_sem=send, recv_sem=recv, device_id=device,
            device_id_type=MESH,
        )

    class Tree:
        def __init__(self, block, rows, recv, send):
            self.block, self.rows, self.recv, self.send = block, rows, recv, send

        def ref(self, q, a, b):
            color, sign = q // 2, 1 - 2 * (q % 2)
            j = at_fs(-sign * (a * (1 - color) + b * color), -sign * (a * color + b * (1 - color)))
            rows = pl.ds(pl.multiple_of(q * self.rows, self.rows), self.rows)
            return self.block(j).at[rows]

        def push(self, q, a, b, da, db):
            color, sign = q // 2, 1 - 2 * (q % 2)
            to = at_fs(sign * (da * (1 - color) + db * color), sign * (da * color + db * (1 - color)))
            ref = self.ref(q, a, b)
            pos = ((a + da) % 4) * 4 + (b + db) % 4
            remote(ref, ref, self.send, self.recv.at[pos], (to, tp)).start()

        def await_(self, a, b):
            ref = self.block(fs)
            pltpu.make_async_copy(ref, ref, self.recv.at[(a % 4) * 4 + b % 4]).wait()

        def each(self, f):
            def go(q, carry):
                f(q)
                return carry

            lax.fori_loop(0, 4, go, 0)

        def run(self, *items):
            for a, b, wait, steps in items:
                if wait:
                    self.await_(a, b)

                def f(q):
                    for da, db in steps:
                        self.push(q, a, b, da, db)

                if steps:
                    self.each(f)

    gup = Tree(lambda j: gu.at[c, j], 352, gsem, ssem.at[1])
    down = Tree(lambda j: dn.at[c, j], 176, dsem, ssem.at[2])

    def across(blocks, recv, send, offsets):
        for dx, dz in offsets:
            j, pos = at_fs(dx, dz), (dx % 4) * 4 + dz % 4
            remote(blocks.at[c, j], blocks.at[c, j], send, recv.at[pos], partner).start()

    def across_wait(blocks, recv, offsets):
        for dx, dz in offsets:
            j, pos = at_fs(dx, dz), (dx % 4) * 4 + dz % 4
            ref = blocks.at[1 - c, j]
            pltpu.make_async_copy(ref, ref, recv.at[pos]).wait()

    NEAR = [(1, 0), (-1, 0), (0, 1), (0, -1)]
    FAR = [(2, 0), (0, 2)]
    DIAG = [(1, 1), (1, -1), (-1, 1), (-1, -1)]
    KNIGHT = [(2, 1), (2, -1), (1, 2), (-1, 2)]
    ALL = [(0, 0)] + NEAR + FAR + DIAG + KNIGHT + [(2, 2)]

    def piece(dy, p):
        return xs.at[(y + dy + 4) % 4, p]

    def piece_out(p):
        remote(piece(0, p), piece(0, p), ssem.at[3], xys.at[p, 0], (fs, at_y(1, c))).start()
        remote(piece(0, p), piece(0, p), ssem.at[3], xys.at[p, 1], (fs, at_y(-1, c))).start()

    def got(ref, sem):
        pltpu.make_async_copy(ref, ref, sem).wait()

    RIGHT, LEFT, UP, DOWN = (1, 0), (-1, 0), (0, 1), (0, -1)
    remote(sv, xs.at[y, c], ssem.at[4], xds.at[0], partner).start()
    piece_out(c)
    for dx, dz in near:
        mine = pw.at[tp, fs]
        remote(mine, mine, ssem.at[0], psem.at[0], (at_fs(dx, dz), tp)).start()
    gup.run((0, 0, False, [RIGHT]))
    gup.run((0, 0, False, [UP]))
    gup.run((0, 0, False, [LEFT]))
    across(gu, gd, ssem.at[5], [(0, 0)])
    across(dn, dd, ssem.at[6], [(0, 0)])

    d, n = iota((512, 512), 0), iota((512, 512), 1)
    perm[...] = ((d % 4) * 128 + d // 4 == n).astype(bf16)
    unperm[...] = ((n % 4) * 128 + n // 4 == d).astype(bf16)
    row, col = iota((LEN, LEN), 0), iota((LEN, LEN), 1)
    for g in range(4):
        band[g] = ((col <= row) & (col > row - 2 ** (g + 1))).astype(bf16)

    got(xs.at[y, 1 - c], xds.at[0])
    piece_out(1 - c)

    three = concat([gv[0], gv[1], gv[2], jnp.zeros((5, 2048), f32)], 0)
    high = three.astype(bf16)
    rest = three - high.astype(f32)
    mid = rest.astype(bf16)
    low = (rest - mid.astype(f32)).astype(bf16)
    for yy in range(4):
        s = slice(512 * yy, 512 * yy + 512)
        moved = sum(jnp.dot(v[:, s], perm[...], preferred_element_type=f32) for v in (low, mid, high))
        for g in range(4):
            gains[g, :, 128 * yy : 128 * yy + 128] = moved[:, 128 * g : 128 * g + 128]
    for core in range(2):
        a = 704 * core
        taps[core, 0] = tv[0, :, a : a + 704]
        taps[core, 1] = tv[1, :, a : a + 704]

    got(pw.at[tp, 0:8], psem.at[0])

    def onward(ox, oz, half, dx, dz):
        ref = pw.at[tp, at_fs(ox, oz), pl.ds(32 * half, 32)]
        remote(ref, ref, ssem.at[0], psem.at[1], (at_fs(dx, dz), tp)).start()

    for o in (0, 1, -1):
        onward(-1, o, 0, 1, 0)
        onward(1, o, 1, -1, 0)
        onward(o, -1, 0, 0, 1)
        onward(o, 1, 1, 0, -1)
    onward(-1, -1, 0, 1, 1)
    onward(1, 1, 1, -1, -1)
    gup.run((1, 0, True, [RIGHT]))
    gup.run((0, 0, False, [DOWN]))
    gup.run((1, 0, False, [UP]))
    got(piece(-1, 0), xys.at[0, 0])
    remote(piece(-1, 0), piece(-1, 0), ssem.at[3], xys.at[0, 2], (fs, at_y(1, c))).start()
    got(piece(1, 1), xys.at[1, 1])
    remote(piece(1, 1), piece(1, 1), ssem.at[3], xys.at[1, 2], (fs, at_y(-1, c))).start()
    got(pw.at[tp, 0:7], psem.at[1])

    def columns(dy, core):
        return pw.at[at_y(dy, core)]

    def pool_across(i, dy):
        remote(columns(dy, c), columns(dy, c), ssem.at[7], pds.at[i], partner).start()

    def half_out(dy, half, sem, to):
        ref = columns(dy, c).at[pl.ds(8 * half, 8)]
        remote(ref, ref, ssem.at[8], pys.at[sem], (fs, at_y(to, c))).start()

    def half_in(dy, half, sem):
        got(columns(dy, c).at[pl.ds(8 * half, 8)], pys.at[sem])

    half_out(0, 0, 0, 1)
    half_out(0, 1, 2, -1)
    half_out(0, 1, 1, 1)
    half_out(0, 0, 3, -1)
    pool_across(0, 0)
    gup.run((2, 0, True, [UP]))
    gup.run((-1, 0, True, [UP]))
    gup.run((0, 1, True, [UP]), (1, 0, False, [DOWN]), (2, 0, False, [DOWN]), (-1, 0, False, [DOWN]))

    acc[...] = jnp.zeros_like(acc)

    def regroup(yy, carry):
        xp = jnp.dot(concat([xs[yy, 0], xs[yy, 1]], 1), perm[...], preferred_element_type=f32)
        at = pl.ds(pl.multiple_of(yy * 128, 128), 128)
        total = acc[...]
        for g in range(4):
            part = xp[:, 128 * g : 128 * g + 128]
            xg[g, :, at] = part.astype(bf16)
            total = total + part * part
        acc[...] = total
        return carry

    def unpack(yy, carry):
        at = pl.ds(pl.multiple_of(yy * 128, 128), 128)
        for p in range(2):
            left = pw[2 * yy, :, 32 * p : 32 * p + 32, :].reshape(512, 128)
            right = pw[2 * yy + 1, :, 32 * p : 32 * p + 32, :].reshape(512, 128)
            wg[2 * p, :, at] = concat([left[:, 0:64], right[:, 0:64]], 1)
            wg[2 * p + 1, :, at] = concat([left[:, 64:128], right[:, 64:128]], 1)
        return carry

    got(piece(1, 0), xys.at[0, 1])
    got(piece(-1, 1), xys.at[1, 0])
    regroup(y, 0)
    regroup((y + 1) % 4, 0)
    regroup((y + 3) % 4, 0)
    gup.run((0, -1, True, []))
    across(gu, gd, ssem.at[5], NEAR)
    gup.run((1, 1, True, [UP]))
    down.run((0, 0, False, [RIGHT]))
    got(columns(0, 1 - c), pds.at[0])
    unpack(y, 0)
    half_in(-1, 0, 0)
    half_out(-1, 0, 4, 1)
    half_in(1, 1, 2)
    half_out(1, 1, 5, -1)
    gup.run((2, 1, True, [UP]))
    got(piece(2, 0), xys.at[0, 2])
    got(piece(2, 1), xys.at[1, 2])
    regroup((y + 2) % 4, 0)
    gup.run((-1, 1, True, [UP]))
    down.run((0, 0, False, [UP]))
    down.run((0, 0, False, [LEFT]))
    down.run((0, 0, False, [DOWN]))
    half_in(-1, 1, 1)
    pool_across(1, -1)
    half_in(1, 0, 3)
    pool_across(2, 1)
    got(columns(-1, 1 - c), pds.at[1])
    unpack((y + 3) % 4, 0)
    got(columns(1, 1 - c), pds.at[2])
    unpack((y + 1) % 4, 0)
    half_in(2, 0, 4)
    half_in(2, 1, 5)
    pool_across(3, 2)
    gup.run((0, 2, True, []))
    across(gu, gd, ssem.at[5], FAR)
    got(columns(2, 1 - c), pds.at[3])
    unpack((y + 2) % 4, 0)

    scale = lax.rsqrt(jnp.sum(acc[...], axis=1, keepdims=True) * (1.0 / 2048) + EPS)
    acc[...] = jnp.zeros_like(acc)
    position = iota((LEN, 512), 0) + 1

    def mix(g, carry):
        divisor = jnp.minimum(position, lax.shift_left(2, g)).astype(f32)
        normed = (xg[g].astype(f32) * scale * gains[g, 0:1, :]).astype(bf16)
        pooled = []
        for s in range(TOK // LEN):
            part = normed[LEN * s : LEN * s + LEN]
            window = jnp.dot(band[g], part, preferred_element_type=f32)
            pooled.append((window / divisor - part.astype(f32)).astype(bf16))
        mixer = jnp.dot(concat(pooled, 0), wg[g], preferred_element_type=f32) * gains[g, 1:2, :]
        middle = (xg[g].astype(f32) + mixer).astype(bf16)
        xg[g] = middle
        total = acc[...]
        for i in range(4):
            part = middle[:, 128 * i : 128 * i + 128].astype(f32)
            total = total + part * part
        acc[...] = total
        return carry

    lax.fori_loop(0, 4, mix, 0)
    scale = lax.rsqrt(jnp.sum(acc[...], axis=1, keepdims=True) * (1.0 / 2048) + EPS)

    def rescale(g, carry):
        xg[g] = (xg[g].astype(f32) * scale * gains[g, 2:3, :]).astype(bf16)
        return carry

    lax.fori_loop(0, 4, rescale, 0)

    def natural(yy, carry):
        at = pl.ds(pl.multiple_of(yy * 128, 128), 128)
        grouped = concat([xg[g, :, at] for g in range(4)], 1)
        moved = jnp.dot(grouped, unperm[...], preferred_element_type=f32).astype(bf16)
        for i in range(4):
            nf[4 * yy + i] = moved[:, 128 * i : 128 * i + 128]
        return carry

    lax.fori_loop(0, 4, natural, 0)

    SETS = ([(0, 0)] + NEAR, FAR + DIAG, KNIGHT + [(2, 2)])
    CHUNKS = ((0, 256), (256, 256), (512, 192))

    def product(core, which, at, width, offsets):
        js = [at_fs(dx, dz) for dx, dz in offsets]
        left = concat([nf[j] for j in js], 1)
        right = concat([gu[core, j, pl.ds(704 * which + at, width), :] for j in js], 1)
        return lax.dot_general(left, right, (((1,), (1,)), ((), ())), preferred_element_type=f32)

    def gather_up(core, i):
        for which in range(2):
            for at, width in CHUNKS:
                part = product(core, which, at, width, SETS[i])
                if i > 0:
                    part = sums[core, which, :, at : at + width] + part
                sums[core, which, :, at : at + width] = part

    def conv(core, which, at, width):
        v = sums[core, which, :, at : at + width] + product(core, which, at, width, SETS[2])
        v = v.astype(bf16).astype(f32)
        k = taps[core, which, :, at : at + width]
        place = iota((TOK, width), 0) % LEN
        back1 = jnp.where(place >= 1, pltpu.roll(v, 1, 0), 0.0)
        back2 = jnp.where(place >= 2, pltpu.roll(v, 2, 0), 0.0)
        return back2 * k[0:1] + back1 * k[1:2] + v * k[2:3]

    def units(core, t):
        at, width = CHUNKS[t]
        a, b = conv(core, 0, at, width), conv(core, 1, at, width)
        hid[core, :, at : at + width] = (a / (1.0 + jnp.exp(-a)) * b).astype(bf16)

    gather_up(c, 0)
    across_wait(gu, gd, SETS[0])
    gather_up(1 - c, 0)
    gup.run((1, -1, True, []), (-1, -1, True, []), (2, -1, True, []))
    across(gu, gd, ssem.at[5], DIAG)
    gather_up(c, 1)
    down.run((1, 0, True, [RIGHT, UP]))
    across_wait(gu, gd, SETS[1])
    gather_up(1 - c, 1)
    gup.run((1, 2, True, []), (2, 2, True, []), (-1, 2, True, []))
    across(gu, gd, ssem.at[5], KNIGHT + [(2, 2)])
    down.run((0, 1, True, [UP]))
    units(c, 0)
    units(c, 1)
    down.run((-1, 0, True, [UP, DOWN]))
    across_wait(gu, gd, SETS[2])
    units(c, 2)
    down.run((0, -1, True, []))
    across(dn, dd, ssem.at[6], NEAR)
    units(1 - c, 0)
    down.run((2, 0, True, [UP]))
    down.run((1, 0, False, [DOWN]), (2, 0, False, [DOWN]))
    units(1 - c, 1)
    down.run((1, 1, True, [UP]))
    down.run((0, 2, True, []))
    across(dn, dd, ssem.at[6], FAR)
    units(1 - c, 2)
    down.run((-1, 1, True, [UP]))

    def pair_of(dz, other):
        cols = x // 2 if other == 0 else 1 - x // 2
        zk = (z + dz + 4) % 4
        return zk * 2 + cols, cols, (zk - y + 4) % 4

    def to_owner(k, h, dy, cols):
        slot, device = (3 - dy) // 2, (fs, at_y(dy, cols))
        remote(pb.at[k, h], rbuf.at[slot, c, h], ssem.at[9], rsem.at[slot, c, h], device).start()

    def hand_on(k, h, cols, role):
        dy = 1 - 2 * h

        @pl.when(role == 2)
        def _():
            there, device = relay_in.at[h, cols], (fs, at_y(dy, c))
            remote(pb.at[k, h], there, ssem.at[9], relsem.at[h, cols], device).start()

        @pl.when(role == 3 - 2 * h)
        def _():
            to_owner(k, h, -dy, cols)

        @pl.when((role == 0) & (cols == c))
        def _():
            rbuf[0, c, h] = pb[k, h]

        @pl.when((role == 0) & (cols != c))
        def _():
            remote(pb.at[k, h], rbuf.at[0, c, h], ssem.at[9], rsem.at[0, c, h], partner).start()

    def part_of(core, k):
        block = concat([dn[core, 2 * k], dn[core, 2 * k + 1]], 1)
        return jnp.dot(hid[core], block, preferred_element_type=f32)

    def own_part(dz, other, at):
        k, cols, role = pair_of(dz, other)
        early[at] = part_of(c, k)

    def columns_done(k, cols, role, total):
        for h in range(2):
            pb[k, h] = total[:, 128 * h : 128 * h + 128].astype(bf16)
        for h in range(2):
            hand_on(k, h, cols, role)

    def owner_columns(dz, other):
        k, cols, role = pair_of(dz, other)
        columns_done(k, cols, role, part_of(c, k) + part_of(1 - c, k))

    def owner_rest(dz, other, at):
        k, cols, role = pair_of(dz, other)
        columns_done(k, cols, role, early[at] + part_of(1 - c, k))

    def owner_half(dz, other, h):
        k, cols, role = pair_of(dz, other)
        total = None
        for core in range(2):
            part = jnp.dot(hid[core], dn[core, 2 * k + h], preferred_element_type=f32)
            total = part if total is None else total + part
        pb[k, h] = total.astype(bf16)
        hand_on(k, h, cols, role)

    def owner_added(dz, other):
        k, cols, role = pair_of(dz, other)
        for h in range(2):

            @pl.when(role == 1 + 2 * h)
            def _():
                got(relay_in.at[h, cols], relsem.at[h, cols])
                pb[k, h] = (pb[k, h].astype(f32) + relay_in[h, cols].astype(f32)).astype(bf16)
                to_owner(k, h, 1 - 2 * h, cols)

    across_wait(dn, dd, [(0, 0)] + NEAR)
    owner_columns(0, 0)
    across_wait(dn, dd, FAR)
    owner_columns(0, 1)
    down.run((2, 1, True, [UP]))
    down.run((1, -1, True, []), (-1, -1, True, []))
    across(dn, dd, ssem.at[6], DIAG)
    own_part(1, 0, 0)
    own_part(-1, 0, 1)
    owner_added(0, 0)
    across_wait(dn, dd, DIAG)
    owner_rest(1, 0, 0)
    owner_rest(-1, 0, 1)
    owner_added(0, 1)
    down.run((2, -1, True, []), (1, 2, True, []), (-1, 2, True, []))
    across(dn, dd, ssem.at[6], KNIGHT)
    own_part(2, 0, 0)
    own_part(1, 1, 1)
    own_part(-1, 1, 2)
    across_wait(dn, dd, KNIGHT)
    owner_rest(2, 0, 0)
    down.run((2, 2, True, []))
    across(dn, dd, ssem.at[6], [(2, 2)])
    owner_half(2, 1, 1 - x % 2)
    owner_rest(1, 1, 1)
    owner_rest(-1, 1, 2)
    across_wait(dn, dd, [(2, 2)])
    owner_half(2, 1, x % 2)
    owner_added(1, 0)
    owner_added(-1, 0)
    owner_added(2, 0)
    owner_added(1, 1)
    owner_added(-1, 1)
    owner_added(2, 1)

    for slot in (1, 2):
        for core in range(2):
            for h in range(2):
                got(rbuf.at[slot, core, h], rsem.at[slot, core, h])
    for h in range(2):
        got(rbuf.at[0, 1 - c, h], rsem.at[0, 1 - c, h])
    for core in range(2):
        for h in range(2):
            total = sum(rbuf[slot, core, h].astype(f32) for slot in range(3))
            out[TOK * core : TOK * core + TOK, 128 * h : 128 * h + 128] = total.astype(bf16)

    for ref, i in (
        (pw.at[0, 0:15], 0), (gu.at[0, 0:15], 1), (dn.at[0, 0:15], 2), (xs.at[0:3], 3), (sv, 4),
        (gu.at[0], 5), (dn.at[0], 6), (pw.at[0:4], 7), (pw.at[0:3], 8), (pb.at[0:7], 9),
    ):
        got(ref, ssem.at[i])


def body(
    stream, gain_mix, pool_weight, pool_gain, gain_ffn, gate_weight, up_weight, gate_taps, up_taps,
    down_weight,
):
    row = lambda v: v.reshape(1, 2048)
    DMA = pltpu.SemaphoreType.DMA
    return pl.pallas_call(
        kernel,
        name="layer",
        out_shape=jax.ShapeDtypeStruct((512, 256), bf16),
        in_specs=[pl.BlockSpec(memory_space=pltpu.HBM)] * 10,
        out_specs=pl.BlockSpec(memory_space=pltpu.VMEM),
        scratch_shapes=[
            pltpu.VMEM((2, 16, 1408, 128), bf16),
            pltpu.VMEM((2, 16, 704, 128), bf16),
            pltpu.VMEM((8, 16, 64, 128), bf16),
            pltpu.VMEM((4, 2, TOK, 256), bf16),
            pltpu.VMEM((TOK, 256), bf16),
            pltpu.VMEM((4, 32, 64), bf16),
            pltpu.VMEM((3, 1, 2048), f32),
            pltpu.VMEM((2, 3, 1408), f32),
            pltpu.VMEM((2, 2, 3, 704), f32),
            pltpu.VMEM((512, 512), bf16),
            pltpu.VMEM((512, 512), bf16),
            pltpu.VMEM((4, LEN, LEN), bf16),
            pltpu.VMEM((4, 8, 512), f32),
            pltpu.VMEM((4, TOK, 512), bf16),
            pltpu.VMEM((4, 512, 512), bf16),
            pltpu.VMEM((16, TOK, 128), bf16),
            pltpu.VMEM((TOK, 128), f32),
            pltpu.VMEM((2, TOK, 704), bf16),
            pltpu.VMEM((8, 2, TOK, 128), bf16),
            pltpu.VMEM((3, 2, 2, TOK, 128), bf16),
            pltpu.VMEM((2, 2, TOK, 704), f32),
            pltpu.VMEM((2, 2, TOK, 128), bf16),
            pltpu.VMEM((3, TOK, 256), f32),
            DMA((11,)),
            DMA((16,)),
            DMA((16,)),
            DMA((2,)),
            DMA((16,)),
            DMA((16,)),
            DMA((6,)),
            DMA((4,)),
            DMA((2, 3)),
            DMA((1,)),
            DMA((3, 2, 2)),
            DMA((10,)),
            DMA((2, 2)),
        ],
        compiler_params=pltpu.CompilerParams(
            collective_id=0, has_side_effects=True, vmem_limit_bytes=60 * 1024 * 1024
        ),
    )(
        stream, row(gain_mix), pool_weight, row(pool_gain), row(gain_ffn), gate_weight.T, up_weight.T,
        gate_taps, up_taps, down_weight,
    )


def solution(mesh):
    return jax.shard_map(
        body,
        mesh=mesh,
        in_specs=(
            P("fs", "tp"), P(), P(None, "fs", "tp"), P(), P(), P("fs", "tp"), P("fs", "tp"), P(), P(),
            P("tp", "fs"),
        ),
        out_specs=P("fs", "tp"),
        check_vma=False,
    )
```

```python
import jax
import jax.numpy as jnp
from jax import lax
from jax.experimental import pallas as pl
from jax.experimental.pallas import tpu as pltpu
from jax.sharding import PartitionSpec as P

MESH = pl.DeviceIdType.MESH
bf16, f32 = jnp.bfloat16, jnp.float32
EPS = 1e-6
LEN = 128
TOK = 256


def concat(parts, axis):
    return jnp.concatenate(parts, axis=axis)


def iota(shape, dim):
    return lax.broadcasted_iota(jnp.int32, shape, dim)


def kernel(
    stream, gain_mix, pool_weight, pool_gain, gain_ffn, gate_weight, up_weight, gate_taps, up_taps,
    down_weight,
    out,
    gu, dn, pw, xs, sv, pv, gv, tv, taps, perm, unperm, band, gains, xg, wg, nf, acc, hid,
    pb, rbuf, sums, relay_in, early,
    lsem, gsem, dsem, psem, gd, dd, pys, pds, xys, xds, rsem, ssem, relsem,
):
    fs, tp = lax.axis_index("fs"), lax.axis_index("tp")
    z, x = fs // 4, fs % 4
    y, c = tp // 2, tp % 2

    def at_fs(dx, dz):
        return ((z + dz + 4) % 4) * 4 + (x + dx + 4) % 4

    def at_y(dy, core):
        return ((y + dy + 4) % 4) * 2 + core

    partner = (fs, y * 2 + (1 - c))

    barrier = pltpu.get_barrier_semaphore()
    near = [(dx, dz) for dz in (0, 1, -1) for dx in (0, 1, -1)][1:]
    peers = [(at_fs(dx, dz), tp) for dx, dz in near]
    peers += [(fs, at_y(dy, core)) for dy in (1, -1) for core in (0, 1)] + [partner]
    for peer in peers:
        pl.semaphore_signal(barrier, inc=1, device_id=peer, device_id_type=MESH)

    loads = [
        (pool_weight, pv),
        (gate_weight, gu.at[c, fs, pl.ds(0, 704)]),
        (up_weight, gu.at[c, fs, pl.ds(704, 704)]),
        (down_weight, dn.at[c, fs]),
        (stream.at[pl.ds(pl.multiple_of(c * TOK, TOK), TOK)], xs.at[y, c]),
        (stream.at[pl.ds(pl.multiple_of((1 - c) * TOK, TOK), TOK)], sv),
        (gain_mix, gv.at[0]),
        (pool_gain, gv.at[1]),
        (gain_ffn, gv.at[2]),
        (gate_taps.at[:, pl.ds(pl.multiple_of(y * 1408, 128), 1408)], tv.at[0]),
        (up_taps.at[:, pl.ds(pl.multiple_of(y * 1408, 128), 1408)], tv.at[1]),
    ]
    loads = [pltpu.make_async_copy(a, b, lsem.at[i]) for i, (a, b) in enumerate(loads)]
    for load in loads:
        load.start()
    loads[0].wait()
    for p in range(2):
        pw[tp, fs, 32 * p : 32 * p + 32, :] = concat([pv[2 * p], pv[2 * p + 1]], 1)
    for load in loads[1:]:
        load.wait()
    pl.semaphore_wait(barrier, len(peers))

    def remote(src, dst, send, recv, device):
        return pltpu.make_async_remote_copy(
            src_ref=src, dst_ref=dst, send_sem=send, recv_sem=recv, device_id=device,
            device_id_type=MESH,
        )

    class Tree:
        def __init__(self, block, rows, recv, send, cross, cross_send):
            self.block, self.rows, self.recv, self.send = block, rows, recv, send
            self.cross, self.cross_send = cross, cross_send

        def ref(self, q, a, b):
            color, sign = q // 2, 1 - 2 * (q % 2)
            j = at_fs(-sign * (a * (1 - color) + b * color), -sign * (a * color + b * (1 - color)))
            rows = pl.ds(pl.multiple_of(q * self.rows, self.rows), self.rows)
            return self.block(j).at[rows]

        def push(self, q, a, b, da, db):
            color, sign = q // 2, 1 - 2 * (q % 2)
            to = at_fs(sign * (da * (1 - color) + db * color), sign * (da * color + db * (1 - color)))
            ref = self.ref(q, a, b)
            pos = ((a + da) % 4) * 4 + (b + db) % 4
            remote(ref, ref, self.send, self.recv.at[pos], (to, tp)).start()

        def await_(self, a, b):
            ref = self.block(fs)
            pltpu.make_async_copy(ref, ref, self.recv.at[(a % 4) * 4 + b % 4]).wait()

        def each(self, f):
            def go(q, carry):
                f(q)
                return carry

            lax.fori_loop(0, 4, go, 0)

        def run(self, *items):
            for a, b, wait, steps in items:
                if wait:
                    self.await_(a, b)

                def f(q):
                    for da, db in steps:
                        self.push(q, a, b, da, db)
                    if wait:
                        ref = self.ref(q, a, b)
                        pos = (a % 4) * 4 + b % 4
                        remote(ref, ref, self.cross_send, self.cross.at[pos], partner).start()

                self.each(f)

    gup = Tree(lambda j: gu.at[c, j], 352, gsem, ssem.at[1], gd, ssem.at[5])
    down = Tree(lambda j: dn.at[c, j], 176, dsem, ssem.at[2], dd, ssem.at[6])

    def across(blocks, recv, send):
        remote(blocks.at[c, fs], blocks.at[c, fs], send, recv.at[0], partner).start()

    def across_wait(blocks, recv, steps):
        for a, b in steps:
            ref = blocks.at[1 - c, fs]
            pltpu.make_async_copy(ref, ref, recv.at[(a % 4) * 4 + b % 4]).wait()

    NEAR = [(1, 0), (-1, 0), (0, 1), (0, -1)]
    FAR = [(2, 0), (0, 2)]
    DIAG = [(1, 1), (1, -1), (-1, 1), (-1, -1)]
    KNIGHT = [(2, 1), (2, -1), (1, 2), (-1, 2)]
    ALL = [(0, 0)] + NEAR + FAR + DIAG + KNIGHT + [(2, 2)]

    def piece(dy, p):
        return xs.at[(y + dy + 4) % 4, p]

    def piece_out(p):
        remote(piece(0, p), piece(0, p), ssem.at[3], xys.at[p, 0], (fs, at_y(1, c))).start()
        remote(piece(0, p), piece(0, p), ssem.at[3], xys.at[p, 1], (fs, at_y(-1, c))).start()

    def got(ref, sem):
        pltpu.make_async_copy(ref, ref, sem).wait()

    RIGHT, LEFT, UP, DOWN = (1, 0), (-1, 0), (0, 1), (0, -1)
    remote(sv, xs.at[y, c], ssem.at[4], xds.at[0], partner).start()
    piece_out(c)
    for dx, dz in near:
        mine = pw.at[tp, fs]
        remote(mine, mine, ssem.at[0], psem.at[0], (at_fs(dx, dz), tp)).start()
    gup.run((0, 0, False, [RIGHT]))
    gup.run((0, 0, False, [UP]))
    gup.run((0, 0, False, [LEFT]))
    across(gu, gd, ssem.at[5])
    across(dn, dd, ssem.at[6])

    d, n = iota((512, 512), 0), iota((512, 512), 1)
    perm[...] = ((d % 4) * 128 + d // 4 == n).astype(bf16)
    unperm[...] = ((n % 4) * 128 + n // 4 == d).astype(bf16)
    row, col = iota((LEN, LEN), 0), iota((LEN, LEN), 1)
    for g in range(4):
        band[g] = ((col <= row) & (col > row - 2 ** (g + 1))).astype(bf16)

    got(xs.at[y, 1 - c], xds.at[0])
    piece_out(1 - c)

    three = concat([gv[0], gv[1], gv[2], jnp.zeros((5, 2048), f32)], 0)
    high = three.astype(bf16)
    rest = three - high.astype(f32)
    mid = rest.astype(bf16)
    low = (rest - mid.astype(f32)).astype(bf16)
    for yy in range(4):
        s = slice(512 * yy, 512 * yy + 512)
        moved = sum(jnp.dot(v[:, s], perm[...], preferred_element_type=f32) for v in (low, mid, high))
        for g in range(4):
            gains[g, :, 128 * yy : 128 * yy + 128] = moved[:, 128 * g : 128 * g + 128]
    for core in range(2):
        a = 704 * core
        taps[core, 0] = tv[0, :, a : a + 704]
        taps[core, 1] = tv[1, :, a : a + 704]

    got(pw.at[tp, 0:8], psem.at[0])

    def onward(ox, oz, half, dx, dz):
        ref = pw.at[tp, at_fs(ox, oz), pl.ds(32 * half, 32)]
        remote(ref, ref, ssem.at[0], psem.at[1], (at_fs(dx, dz), tp)).start()

    for o in (0, 1, -1):
        onward(-1, o, 0, 1, 0)
        onward(1, o, 1, -1, 0)
        onward(o, -1, 0, 0, 1)
        onward(o, 1, 1, 0, -1)
    onward(-1, -1, 0, 1, 1)
    onward(1, 1, 1, -1, -1)
    gup.run((1, 0, True, [RIGHT]))
    gup.run((0, 0, False, [DOWN]))
    gup.run((1, 0, False, [UP]))
    got(piece(-1, 0), xys.at[0, 0])
    remote(piece(-1, 0), piece(-1, 0), ssem.at[3], xys.at[0, 2], (fs, at_y(1, c))).start()
    got(piece(1, 1), xys.at[1, 1])
    remote(piece(1, 1), piece(1, 1), ssem.at[3], xys.at[1, 2], (fs, at_y(-1, c))).start()
    got(pw.at[tp, 0:7], psem.at[1])

    def columns(dy, core):
        return pw.at[at_y(dy, core)]

    def pool_across(i, dy):
        remote(columns(dy, c), columns(dy, c), ssem.at[7], pds.at[i], partner).start()

    def half_out(dy, half, sem, to):
        ref = columns(dy, c).at[pl.ds(8 * half, 8)]
        remote(ref, ref, ssem.at[8], pys.at[sem], (fs, at_y(to, c))).start()

    def half_in(dy, half, sem):
        got(columns(dy, c).at[pl.ds(8 * half, 8)], pys.at[sem])

    half_out(0, 0, 0, 1)
    half_out(0, 1, 2, -1)
    half_out(0, 1, 1, 1)
    half_out(0, 0, 3, -1)
    pool_across(0, 0)
    gup.run((2, 0, True, [UP]))
    gup.run((-1, 0, True, [UP]))
    gup.run((0, 1, True, [UP]), (1, 0, False, [DOWN]), (2, 0, False, [DOWN]), (-1, 0, False, [DOWN]))

    acc[...] = jnp.zeros_like(acc)

    def regroup(yy, carry):
        xp = jnp.dot(concat([xs[yy, 0], xs[yy, 1]], 1), perm[...], preferred_element_type=f32)
        at = pl.ds(pl.multiple_of(yy * 128, 128), 128)
        total = acc[...]
        for g in range(4):
            part = xp[:, 128 * g : 128 * g + 128]
            xg[g, :, at] = part.astype(bf16)
            total = total + part * part
        acc[...] = total
        return carry

    def unpack(yy, carry):
        at = pl.ds(pl.multiple_of(yy * 128, 128), 128)
        for p in range(2):
            left = pw[2 * yy, :, 32 * p : 32 * p + 32, :].reshape(512, 128)
            right = pw[2 * yy + 1, :, 32 * p : 32 * p + 32, :].reshape(512, 128)
            wg[2 * p, :, at] = concat([left[:, 0:64], right[:, 0:64]], 1)
            wg[2 * p + 1, :, at] = concat([left[:, 64:128], right[:, 64:128]], 1)
        return carry

    got(piece(1, 0), xys.at[0, 1])
    got(piece(-1, 1), xys.at[1, 0])
    regroup(y, 0)
    regroup((y + 1) % 4, 0)
    regroup((y + 3) % 4, 0)
    gup.run((0, -1, True, []))
    gup.run((1, 1, True, [UP]))
    down.run((0, 0, False, [RIGHT]))
    got(columns(0, 1 - c), pds.at[0])
    unpack(y, 0)
    half_in(-1, 0, 0)
    half_out(-1, 0, 4, 1)
    half_in(1, 1, 2)
    half_out(1, 1, 5, -1)
    gup.run((2, 1, True, [UP]))
    got(piece(2, 0), xys.at[0, 2])
    got(piece(2, 1), xys.at[1, 2])
    regroup((y + 2) % 4, 0)
    gup.run((-1, 1, True, [UP]))
    down.run((0, 0, False, [UP]))
    down.run((0, 0, False, [LEFT]))
    down.run((0, 0, False, [DOWN]))
    half_in(-1, 1, 1)
    pool_across(1, -1)
    half_in(1, 0, 3)
    pool_across(2, 1)
    got(columns(-1, 1 - c), pds.at[1])
    unpack((y + 3) % 4, 0)
    got(columns(1, 1 - c), pds.at[2])
    unpack((y + 1) % 4, 0)
    half_in(2, 0, 4)
    half_in(2, 1, 5)
    pool_across(3, 2)
    gup.run((0, 2, True, []))
    got(columns(2, 1 - c), pds.at[3])
    unpack((y + 2) % 4, 0)

    scale = lax.rsqrt(jnp.sum(acc[...], axis=1, keepdims=True) * (1.0 / 2048) + EPS)
    acc[...] = jnp.zeros_like(acc)
    position = iota((LEN, 512), 0) + 1

    def mix(g, carry):
        divisor = jnp.minimum(position, lax.shift_left(2, g)).astype(f32)
        normed = (xg[g].astype(f32) * scale * gains[g, 0:1, :]).astype(bf16)
        pooled = []
        for s in range(TOK // LEN):
            part = normed[LEN * s : LEN * s + LEN]
            window = jnp.dot(band[g], part, preferred_element_type=f32)
            pooled.append((window / divisor - part.astype(f32)).astype(bf16))
        mixer = jnp.dot(concat(pooled, 0), wg[g], preferred_element_type=f32) * gains[g, 1:2, :]
        middle = (xg[g].astype(f32) + mixer).astype(bf16)
        xg[g] = middle
        total = acc[...]
        for i in range(4):
            part = middle[:, 128 * i : 128 * i + 128].astype(f32)
            total = total + part * part
        acc[...] = total
        return carry

    lax.fori_loop(0, 4, mix, 0)
    scale = lax.rsqrt(jnp.sum(acc[...], axis=1, keepdims=True) * (1.0 / 2048) + EPS)

    def rescale(g, carry):
        xg[g] = (xg[g].astype(f32) * scale * gains[g, 2:3, :]).astype(bf16)
        return carry

    lax.fori_loop(0, 4, rescale, 0)

    def natural(yy, carry):
        at = pl.ds(pl.multiple_of(yy * 128, 128), 128)
        grouped = concat([xg[g, :, at] for g in range(4)], 1)
        moved = jnp.dot(grouped, unperm[...], preferred_element_type=f32).astype(bf16)
        for i in range(4):
            nf[4 * yy + i] = moved[:, 128 * i : 128 * i + 128]
        return carry

    lax.fori_loop(0, 4, natural, 0)

    SETS = ([(0, 0)] + NEAR, FAR + DIAG, KNIGHT + [(2, 2)])
    CHUNKS = ((0, 256), (256, 256), (512, 192))

    def product(core, which, at, width, offsets):
        js = [at_fs(dx, dz) for dx, dz in offsets]
        left = concat([nf[j] for j in js], 1)
        right = concat([gu[core, j, pl.ds(704 * which + at, width), :] for j in js], 1)
        return lax.dot_general(left, right, (((1,), (1,)), ((), ())), preferred_element_type=f32)

    def gather_up(core, i):
        for which in range(2):
            for at, width in CHUNKS:
                part = product(core, which, at, width, SETS[i])
                if i > 0:
                    part = sums[core, which, :, at : at + width] + part
                sums[core, which, :, at : at + width] = part

    def conv(core, which, at, width):
        v = sums[core, which, :, at : at + width] + product(core, which, at, width, SETS[2])
        v = v.astype(bf16).astype(f32)
        k = taps[core, which, :, at : at + width]
        place = iota((TOK, width), 0) % LEN
        back1 = jnp.where(place >= 1, pltpu.roll(v, 1, 0), 0.0)
        back2 = jnp.where(place >= 2, pltpu.roll(v, 2, 0), 0.0)
        return back2 * k[0:1] + back1 * k[1:2] + v * k[2:3]

    def units(core, t):
        at, width = CHUNKS[t]
        a, b = conv(core, 0, at, width), conv(core, 1, at, width)
        hid[core, :, at : at + width] = (a / (1.0 + jnp.exp(-a)) * b).astype(bf16)

    gather_up(c, 0)
    across_wait(gu, gd, SETS[0])
    gather_up(1 - c, 0)
    gup.run((1, -1, True, []), (-1, -1, True, []), (2, -1, True, []))
    gather_up(c, 1)
    down.run((1, 0, True, [RIGHT, UP]))
    across_wait(gu, gd, SETS[1])
    gather_up(1 - c, 1)
    gup.run((1, 2, True, []), (2, 2, True, []), (-1, 2, True, []))
    down.run((0, 1, True, [UP]))
    units(c, 0)
    units(c, 1)
    down.run((-1, 0, True, [UP, DOWN]))
    across_wait(gu, gd, SETS[2])
    units(c, 2)
    down.run((0, -1, True, []))
    units(1 - c, 0)
    down.run((2, 0, True, [UP]))
    down.run((1, 0, False, [DOWN]), (2, 0, False, [DOWN]))
    units(1 - c, 1)
    down.run((1, 1, True, [UP]))
    down.run((0, 2, True, []))
    units(1 - c, 2)
    down.run((-1, 1, True, [UP]))

    def pair_of(dz, other):
        cols = x // 2 if other == 0 else 1 - x // 2
        zk = (z + dz + 4) % 4
        return zk * 2 + cols, cols, (zk - y + 4) % 4

    def to_owner(k, h, dy, cols):
        slot, device = (3 - dy) // 2, (fs, at_y(dy, cols))
        remote(pb.at[k, h], rbuf.at[slot, c, h], ssem.at[9], rsem.at[slot, c, h], device).start()

    def hand_on(k, h, cols, role):
        dy = 1 - 2 * h

        @pl.when(role == 2)
        def _():
            there, device = relay_in.at[h, cols], (fs, at_y(dy, c))
            remote(pb.at[k, h], there, ssem.at[9], relsem.at[h, cols], device).start()

        @pl.when(role == 3 - 2 * h)
        def _():
            to_owner(k, h, -dy, cols)

        @pl.when((role == 0) & (cols == c))
        def _():
            rbuf[0, c, h] = pb[k, h]

        @pl.when((role == 0) & (cols != c))
        def _():
            remote(pb.at[k, h], rbuf.at[0, c, h], ssem.at[9], rsem.at[0, c, h], partner).start()

    def part_of(core, k):
        block = concat([dn[core, 2 * k], dn[core, 2 * k + 1]], 1)
        return jnp.dot(hid[core], block, preferred_element_type=f32)

    def own_part(dz, other, at):
        k, cols, role = pair_of(dz, other)
        early[at] = part_of(c, k)

    def columns_done(k, cols, role, total):
        for h in range(2):
            pb[k, h] = total[:, 128 * h : 128 * h + 128].astype(bf16)
        for h in range(2):
            hand_on(k, h, cols, role)

    def owner_columns(dz, other):
        k, cols, role = pair_of(dz, other)
        columns_done(k, cols, role, part_of(c, k) + part_of(1 - c, k))

    def owner_rest(dz, other, at):
        k, cols, role = pair_of(dz, other)
        columns_done(k, cols, role, early[at] + part_of(1 - c, k))

    def owner_added(dz, other):
        k, cols, role = pair_of(dz, other)
        for h in range(2):

            @pl.when(role == 1 + 2 * h)
            def _():
                got(relay_in.at[h, cols], relsem.at[h, cols])
                pb[k, h] = (pb[k, h].astype(f32) + relay_in[h, cols].astype(f32)).astype(bf16)
                to_owner(k, h, 1 - 2 * h, cols)

    across_wait(dn, dd, [(0, 0)] + NEAR)
    owner_columns(0, 0)
    across_wait(dn, dd, FAR)
    owner_columns(0, 1)
    down.run((2, 1, True, [UP]))
    down.run((1, -1, True, []), (-1, -1, True, []))
    own_part(1, 0, 0)
    own_part(-1, 0, 1)
    owner_added(0, 0)
    across_wait(dn, dd, DIAG)
    owner_rest(1, 0, 0)
    owner_rest(-1, 0, 1)
    owner_added(0, 1)
    down.run((2, -1, True, []), (1, 2, True, []), (-1, 2, True, []))
    own_part(2, 0, 0)
    own_part(1, 1, 1)
    own_part(-1, 1, 2)
    across_wait(dn, dd, KNIGHT)
    owner_rest(2, 0, 0)
    down.run((2, 2, True, []))
    owner_rest(1, 1, 1)
    owner_rest(-1, 1, 2)
    own_part(2, 1, 0)
    across_wait(dn, dd, [(2, 2)])
    owner_rest(2, 1, 0)
    owner_added(1, 0)
    owner_added(-1, 0)
    owner_added(2, 0)
    owner_added(1, 1)
    owner_added(-1, 1)
    owner_added(2, 1)

    for slot in (1, 2):
        for core in range(2):
            for h in range(2):
                got(rbuf.at[slot, core, h], rsem.at[slot, core, h])
    for h in range(2):
        got(rbuf.at[0, 1 - c, h], rsem.at[0, 1 - c, h])
    for core in range(2):
        for h in range(2):
            total = sum(rbuf[slot, core, h].astype(f32) for slot in range(3))
            out[TOK * core : TOK * core + TOK, 128 * h : 128 * h + 128] = total.astype(bf16)

    for ref, i in (
        (pw.at[0, 0:15], 0), (gu.at[0, 0:15], 1), (dn.at[0, 0:15], 2), (xs.at[0:3], 3), (sv, 4),
        (gu.at[0], 5), (dn.at[0], 6), (pw.at[0:4], 7), (pw.at[0:3], 8), (pb.at[0:7], 9),
    ):
        got(ref, ssem.at[i])


def body(
    stream, gain_mix, pool_weight, pool_gain, gain_ffn, gate_weight, up_weight, gate_taps, up_taps,
    down_weight,
):
    row = lambda v: v.reshape(1, 2048)
    DMA = pltpu.SemaphoreType.DMA
    return pl.pallas_call(
        kernel,
        name="layer",
        out_shape=jax.ShapeDtypeStruct((512, 256), bf16),
        in_specs=[pl.BlockSpec(memory_space=pltpu.HBM)] * 10,
        out_specs=pl.BlockSpec(memory_space=pltpu.VMEM),
        scratch_shapes=[
            pltpu.VMEM((2, 16, 1408, 128), bf16),
            pltpu.VMEM((2, 16, 704, 128), bf16),
            pltpu.VMEM((8, 16, 64, 128), bf16),
            pltpu.VMEM((4, 2, TOK, 256), bf16),
            pltpu.VMEM((TOK, 256), bf16),
            pltpu.VMEM((4, 32, 64), bf16),
            pltpu.VMEM((3, 1, 2048), f32),
            pltpu.VMEM((2, 3, 1408), f32),
            pltpu.VMEM((2, 2, 3, 704), f32),
            pltpu.VMEM((512, 512), bf16),
            pltpu.VMEM((512, 512), bf16),
            pltpu.VMEM((4, LEN, LEN), bf16),
            pltpu.VMEM((4, 8, 512), f32),
            pltpu.VMEM((4, TOK, 512), bf16),
            pltpu.VMEM((4, 512, 512), bf16),
            pltpu.VMEM((16, TOK, 128), bf16),
            pltpu.VMEM((TOK, 128), f32),
            pltpu.VMEM((2, TOK, 704), bf16),
            pltpu.VMEM((8, 2, TOK, 128), bf16),
            pltpu.VMEM((3, 2, 2, TOK, 128), bf16),
            pltpu.VMEM((2, 2, TOK, 704), f32),
            pltpu.VMEM((2, 2, TOK, 128), bf16),
            pltpu.VMEM((3, TOK, 256), f32),
            DMA((11,)),
            DMA((16,)),
            DMA((16,)),
            DMA((2,)),
            DMA((16,)),
            DMA((16,)),
            DMA((6,)),
            DMA((4,)),
            DMA((2, 3)),
            DMA((1,)),
            DMA((3, 2, 2)),
            DMA((10,)),
            DMA((2, 2)),
        ],
        compiler_params=pltpu.CompilerParams(
            collective_id=0, has_side_effects=True, vmem_limit_bytes=50 * 1024 * 1024
        ),
    )(
        *[pltpu.with_memory_space_constraint(v, pltpu.HBM) for v in (
        stream, row(gain_mix), pool_weight, row(pool_gain), row(gain_ffn), gate_weight.T, up_weight.T,
        gate_taps, up_taps, down_weight)]
    )


def solution(mesh):
    return jax.shard_map(
        body,
        mesh=mesh,
        in_specs=(
            P("fs", "tp"), P(), P(None, "fs", "tp"), P(), P(), P("fs", "tp"), P("fs", "tp"), P(), P(),
            P("tp", "fs"),
        ),
        out_specs=P("fs", "tp"),
        check_vma=False,
    )
```

```python
import jax
import jax.numpy as jnp
from jax import lax
from jax.experimental import pallas as pl
from jax.experimental.pallas import tpu as pltpu
from jax.sharding import PartitionSpec as P

MESH = pl.DeviceIdType.MESH
bf16, f32 = jnp.bfloat16, jnp.float32
EPS = 1e-6
LEN = 128
PIECES = (0, 1)
TOK = 256


def concat(parts, axis):
    return jnp.concatenate(parts, axis=axis)


def iota(shape, dim):
    return lax.broadcasted_iota(jnp.int32, shape, dim)


def kernel(
    stream, gain_mix, pool_weight, pool_gain, gain_ffn, gate_weight, up_weight, gate_taps, up_taps,
    down_weight,
    out,
    gu, dn, pw, xs, sv, pv, gv, tv, taps, perm, unperm, band, gains, xg, wg, nf, acc, hid,
    pb, rbuf, sums, relay_in, early,
    lsem, gsem, dsem, psem, gd, dd, pys, pds, xys, xds, rsem, ssem, relsem,
):
    fs, tp = lax.axis_index("fs"), lax.axis_index("tp")
    z, x = fs // 4, fs % 4
    y, c = tp // 2, tp % 2

    def at_fs(dx, dz):
        return ((z + dz + 4) % 4) * 4 + (x + dx + 4) % 4

    def at_y(dy, core):
        return ((y + dy + 4) % 4) * 2 + core

    partner = (fs, y * 2 + (1 - c))

    barrier = pltpu.get_barrier_semaphore()
    near = [(dx, dz) for dz in (0, 1, -1) for dx in (0, 1, -1)][1:]
    peers = [(at_fs(dx, dz), tp) for dx, dz in near]
    peers += [(fs, at_y(dy, core)) for dy in (1, -1) for core in (0, 1)] + [partner]
    for peer in peers:
        pl.semaphore_signal(barrier, inc=1, device_id=peer, device_id_type=MESH)

    loads = [
        (pool_weight, pv),
        (gate_weight, gu.at[c, fs, pl.ds(0, 704)]),
        (up_weight, gu.at[c, fs, pl.ds(704, 704)]),
        (stream.at[pl.ds(pl.multiple_of(c * TOK, TOK), TOK)], xs.at[y, c]),
        (stream.at[pl.ds(pl.multiple_of((1 - c) * TOK, TOK), TOK)], sv),
        (down_weight, dn.at[c, fs]),
        (gain_mix, gv.at[0]),
        (pool_gain, gv.at[1]),
        (gain_ffn, gv.at[2]),
        (gate_taps.at[:, pl.ds(pl.multiple_of(y * 1408, 128), 1408)], tv.at[0]),
        (up_taps.at[:, pl.ds(pl.multiple_of(y * 1408, 128), 1408)], tv.at[1]),
    ]
    loads = [pltpu.make_async_copy(a, b, lsem.at[i]) for i, (a, b) in enumerate(loads)]
    for load in loads:
        load.start()
    loads[0].wait()
    for p in range(2):
        pw[tp, fs, 32 * p : 32 * p + 32, :] = concat([pv[2 * p], pv[2 * p + 1]], 1)
    for load in loads[1:5]:
        load.wait()
    pl.semaphore_wait(barrier, len(peers))

    def remote(src, dst, send, recv, device):
        return pltpu.make_async_remote_copy(
            src_ref=src, dst_ref=dst, send_sem=send, recv_sem=recv, device_id=device,
            device_id_type=MESH,
        )

    def got(ref, sem):
        pltpu.make_async_copy(ref, ref, sem).wait()

    def group(a, b):
        return {0: 0, 1: 0, 4: 1, 2: 2, 5: 3, 8: 4}[a * a + b * b]

    class Tree:
        def __init__(self, block, rows, recv, send, cross, cross_send):
            self.block, self.rows, self.recv, self.send = block, rows, recv, send
            self.cross, self.cross_send = cross, cross_send

        def ref(self, q, a, b):
            color, sign = q // 2, 1 - 2 * (q % 2)
            j = at_fs(-sign * (a * (1 - color) + b * color), -sign * (a * color + b * (1 - color)))
            rows = pl.ds(pl.multiple_of(q * self.rows, self.rows), self.rows)
            return self.block(j).at[rows]

        def push(self, q, a, b, da, db):
            color, sign = q // 2, 1 - 2 * (q % 2)
            to = at_fs(sign * (da * (1 - color) + db * color), sign * (da * color + db * (1 - color)))
            ref = self.ref(q, a, b)
            pos = ((a + da) % 4) * 4 + (b + db) % 4
            remote(ref, ref, self.send, self.recv.at[pos], (to, tp)).start()

        def await_(self, a, b):
            ref = self.block(fs)
            pltpu.make_async_copy(ref, ref, self.recv.at[(a % 4) * 4 + b % 4]).wait()

        def each(self, f):
            def go(q, carry):
                f(q)
                return carry

            lax.fori_loop(0, 4, go, 0)

        def run(self, *items):
            for a, b, wait, steps in items:
                if wait:
                    self.await_(a, b)

                def f(q):
                    for da, db in steps:
                        self.push(q, a, b, da, db)
                    if wait:
                        ref = self.ref(q, a, b)
                        sem = self.cross.at[group(a, b)]
                        remote(ref, ref, self.cross_send, sem, partner).start()

                self.each(f)

    gup = Tree(lambda j: gu.at[c, j], 352, gsem, ssem.at[1], gd, ssem.at[5])
    down = Tree(lambda j: dn.at[c, j], 176, dsem, ssem.at[2], dd, ssem.at[6])

    def across(blocks, recv, send):
        remote(blocks.at[c, fs], blocks.at[c, fs], send, recv.at[0], partner).start()

    def across_wait(blocks, recv, i):
        count = (5, 2, 4, 4, 1)[i]
        got(blocks.at[1 - c, 0:count], recv.at[i])

    NEAR = [(1, 0), (-1, 0), (0, 1), (0, -1)]
    FAR = [(2, 0), (0, 2)]
    DIAG = [(1, 1), (1, -1), (-1, 1), (-1, -1)]
    KNIGHT = [(2, 1), (2, -1), (1, 2), (-1, 2)]

    def piece(dy, p):
        return xs.at[(y + dy + 4) % 4, p]

    def piece_out(p):
        remote(piece(0, p), piece(0, p), ssem.at[3], xys.at[p, 0], (fs, at_y(1, c))).start()
        remote(piece(0, p), piece(0, p), ssem.at[3], xys.at[p, 1], (fs, at_y(-1, c))).start()

    RIGHT, LEFT, UP, DOWN = (1, 0), (-1, 0), (0, 1), (0, -1)
    remote(sv, xs.at[y, c], ssem.at[4], xds.at[0], partner).start()
    piece_out(c)
    for dx, dz in near:
        mine = pw.at[tp, fs]
        remote(mine, mine, ssem.at[0], psem.at[0], (at_fs(dx, dz), tp)).start()
    gup.run((0, 0, False, [RIGHT]))
    gup.run((0, 0, False, [UP]))
    gup.run((0, 0, False, [LEFT]))
    across(gu, gd, ssem.at[5])
    for load in loads[5:]:
        load.wait()
    across(dn, dd, ssem.at[6])

    d, n = iota((512, 512), 0), iota((512, 512), 1)
    perm[...] = ((d % 4) * 128 + d // 4 == n).astype(bf16)
    unperm[...] = ((n % 4) * 128 + n // 4 == d).astype(bf16)
    row, col = iota((LEN, LEN), 0), iota((LEN, LEN), 1)
    for g in range(4):
        band[g] = ((col <= row) & (col > row - 2 ** (g + 1))).astype(bf16)

    got(xs.at[y, 1 - c], xds.at[0])
    piece_out(1 - c)

    three = concat([gv[0], gv[1], gv[2], jnp.zeros((5, 2048), f32)], 0)
    high = three.astype(bf16)
    rest = three - high.astype(f32)
    mid = rest.astype(bf16)
    low = (rest - mid.astype(f32)).astype(bf16)
    for yy in range(4):
        s = slice(512 * yy, 512 * yy + 512)
        moved = sum(jnp.dot(v[:, s], perm[...], preferred_element_type=f32) for v in (low, mid, high))
        for g in range(4):
            gains[g, :, 128 * yy : 128 * yy + 128] = moved[:, 128 * g : 128 * g + 128]
    for core in range(2):
        a = 704 * core
        taps[core, 0] = tv[0, :, a : a + 704]
        taps[core, 1] = tv[1, :, a : a + 704]

    got(pw.at[tp, 0:8], psem.at[0])

    def onward(ox, oz, half, dx, dz):
        ref = pw.at[tp, at_fs(ox, oz), pl.ds(32 * half, 32)]
        remote(ref, ref, ssem.at[0], psem.at[1], (at_fs(dx, dz), tp)).start()

    for o in (0, 1, -1):
        onward(-1, o, 0, 1, 0)
        onward(1, o, 1, -1, 0)
        onward(o, -1, 0, 0, 1)
        onward(o, 1, 1, 0, -1)
    onward(-1, -1, 0, 1, 1)
    onward(1, 1, 1, -1, -1)
    gup.run((1, 0, True, [RIGHT]))
    gup.run((0, 0, False, [DOWN]))
    gup.run((1, 0, False, [UP]))
    got(piece(-1, 0), xys.at[0, 0])
    remote(piece(-1, 0), piece(-1, 0), ssem.at[3], xys.at[0, 2], (fs, at_y(1, c))).start()
    got(piece(1, 1), xys.at[1, 1])
    remote(piece(1, 1), piece(1, 1), ssem.at[3], xys.at[1, 2], (fs, at_y(-1, c))).start()
    got(pw.at[tp, 0:7], psem.at[1])

    def columns(dy, core):
        return pw.at[at_y(dy, core)]

    def pool_across(i, dy):
        remote(columns(dy, c), columns(dy, c), ssem.at[7], pds.at[i], partner).start()

    def half_out(dy, half, sem, to):
        ref = columns(dy, c).at[pl.ds(8 * half, 8)]
        remote(ref, ref, ssem.at[8], pys.at[sem], (fs, at_y(to, c))).start()

    def half_in(dy, half, sem):
        got(columns(dy, c).at[pl.ds(8 * half, 8)], pys.at[sem])

    half_out(0, 0, 0, 1)
    half_out(0, 1, 2, -1)
    half_out(0, 1, 1, 1)
    half_out(0, 0, 3, -1)
    pool_across(0, 0)
    gup.run((2, 0, True, [UP]))
    gup.run((-1, 0, True, [UP]))
    gup.run((0, 1, True, [UP]), (1, 0, False, [DOWN]), (2, 0, False, [DOWN]), (-1, 0, False, [DOWN]))

    acc[...] = jnp.zeros_like(acc)

    def regroup(yy, carry):
        xp = jnp.dot(concat([xs[yy, 0], xs[yy, 1]], 1), perm[...], preferred_element_type=f32)
        at = pl.ds(pl.multiple_of(yy * 128, 128), 128)
        total = acc[...]
        for g in range(4):
            part = xp[:, 128 * g : 128 * g + 128]
            xg[g, :, at] = part.astype(bf16)
            total = total + part * part
        acc[...] = total
        return carry

    def unpack(yy, carry):
        at = pl.ds(pl.multiple_of(yy * 128, 128), 128)
        for p in range(2):
            left = pw[2 * yy, :, 32 * p : 32 * p + 32, :].reshape(512, 128)
            right = pw[2 * yy + 1, :, 32 * p : 32 * p + 32, :].reshape(512, 128)
            wg[2 * p, :, at] = concat([left[:, 0:64], right[:, 0:64]], 1)
            wg[2 * p + 1, :, at] = concat([left[:, 64:128], right[:, 64:128]], 1)
        return carry

    got(piece(1, 0), xys.at[0, 1])
    got(piece(-1, 1), xys.at[1, 0])
    regroup(y, 0)
    regroup((y + 1) % 4, 0)
    regroup((y + 3) % 4, 0)
    gup.run((0, -1, True, []))
    gup.run((1, 1, True, [UP]))
    down.run((0, 0, False, [RIGHT]))
    got(columns(0, 1 - c), pds.at[0])
    unpack(y, 0)
    half_in(-1, 0, 0)
    half_out(-1, 0, 4, 1)
    half_in(1, 1, 2)
    half_out(1, 1, 5, -1)
    gup.run((2, 1, True, [UP]))
    got(piece(2, 0), xys.at[0, 2])
    got(piece(2, 1), xys.at[1, 2])
    regroup((y + 2) % 4, 0)
    gup.run((-1, 1, True, [UP]))
    down.run((0, 0, False, [UP]))
    down.run((0, 0, False, [LEFT]))
    down.run((0, 0, False, [DOWN]))
    half_in(-1, 1, 1)
    pool_across(1, -1)
    half_in(1, 0, 3)
    pool_across(2, 1)
    got(columns(-1, 1 - c), pds.at[1])
    unpack((y + 3) % 4, 0)
    got(columns(1, 1 - c), pds.at[2])
    unpack((y + 1) % 4, 0)
    half_in(2, 0, 4)
    half_in(2, 1, 5)
    pool_across(3, 2)
    gup.run((0, 2, True, []))
    got(columns(2, 1 - c), pds.at[3])
    unpack((y + 2) % 4, 0)

    scale = lax.rsqrt(jnp.sum(acc[...], axis=1, keepdims=True) * (1.0 / 2048) + EPS)
    acc[...] = jnp.zeros_like(acc)
    position = iota((LEN, 512), 0) + 1

    def mix(g, carry):
        divisor = jnp.minimum(position, lax.shift_left(2, g)).astype(f32)
        normed = (xg[g].astype(f32) * scale * gains[g, 0:1, :]).astype(bf16)
        pooled = []
        for s in range(TOK // LEN):
            part = normed[LEN * s : LEN * s + LEN]
            window = jnp.dot(band[g], part, preferred_element_type=f32)
            pooled.append((window / divisor - part.astype(f32)).astype(bf16))
        mixer = jnp.dot(concat(pooled, 0), wg[g], preferred_element_type=f32) * gains[g, 1:2, :]
        middle = (xg[g].astype(f32) + mixer).astype(bf16)
        xg[g] = middle
        total = acc[...]
        for i in range(4):
            part = middle[:, 128 * i : 128 * i + 128].astype(f32)
            total = total + part * part
        acc[...] = total
        return carry

    lax.fori_loop(0, 4, mix, 0)
    scale = lax.rsqrt(jnp.sum(acc[...], axis=1, keepdims=True) * (1.0 / 2048) + EPS)

    def rescale(g, carry):
        xg[g] = (xg[g].astype(f32) * scale * gains[g, 2:3, :]).astype(bf16)
        return carry

    lax.fori_loop(0, 4, rescale, 0)

    def natural(yy, carry):
        at = pl.ds(pl.multiple_of(yy * 128, 128), 128)
        grouped = concat([xg[g, :, at] for g in range(4)], 1)
        moved = jnp.dot(grouped, unperm[...], preferred_element_type=f32).astype(bf16)
        for i in range(4):
            nf[4 * yy + i] = moved[:, 128 * i : 128 * i + 128]
        return carry

    lax.fori_loop(0, 4, natural, 0)

    SETS = ([(0, 0)] + NEAR, FAR + DIAG, KNIGHT + [(2, 2)])
    CHUNKS = ((0, 256), (256, 256), (512, 192))

    def product(core, which, at, width, offsets):
        js = [at_fs(dx, dz) for dx, dz in offsets]
        left = concat([nf[j] for j in js], 1)
        right = concat([gu[core, j, pl.ds(704 * which + at, width), :] for j in js], 1)
        return lax.dot_general(left, right, (((1,), (1,)), ((), ())), preferred_element_type=f32)

    def gather_up(core, i):
        for which in range(2):
            for at, width in CHUNKS:
                part = product(core, which, at, width, SETS[i])
                if i > 0:
                    part = sums[core, which, :, at : at + width] + part
                sums[core, which, :, at : at + width] = part

    def conv(core, which, at, width):
        v = sums[core, which, :, at : at + width] + product(core, which, at, width, SETS[2])
        v = v.astype(bf16).astype(f32)
        k = taps[core, which, :, at : at + width]
        place = iota((TOK, width), 0) % LEN
        back1 = jnp.where(place >= 1, pltpu.roll(v, 1, 0), 0.0)
        back2 = jnp.where(place >= 2, pltpu.roll(v, 2, 0), 0.0)
        return back2 * k[0:1] + back1 * k[1:2] + v * k[2:3]

    def units(core, t):
        at, width = CHUNKS[t]
        a, b = conv(core, 0, at, width), conv(core, 1, at, width)
        hid[core, :, at : at + width] = (a / (1.0 + jnp.exp(-a)) * b).astype(bf16)

    gather_up(c, 0)
    across_wait(gu, gd, 0)
    gather_up(1 - c, 0)
    gup.run((1, -1, True, []), (-1, -1, True, []), (2, -1, True, []))
    gather_up(c, 1)
    down.run((1, 0, True, [RIGHT, UP]))
    across_wait(gu, gd, 1)
    across_wait(gu, gd, 2)
    gather_up(1 - c, 1)
    gup.run((1, 2, True, []), (2, 2, True, []), (-1, 2, True, []))
    units(c, 0)
    down.run((0, 1, True, [UP]))
    units(c, 1)
    down.run((-1, 0, True, [UP, DOWN]))
    units(c, 2)
    across_wait(gu, gd, 3)
    across_wait(gu, gd, 4)
    units(1 - c, 0)
    down.run((0, -1, True, []))
    units(1 - c, 1)
    down.run((2, 0, True, [UP]))
    down.run((1, 0, False, [DOWN]), (2, 0, False, [DOWN]))
    units(1 - c, 2)
    down.run((1, 1, True, [UP]))

    def pair_of(dz, other):
        cols = x // 2 if other == 0 else 1 - x // 2
        zk = (z + dz + 4) % 4
        return zk * 2 + cols, cols, (zk - y + 4) % 4

    def to_owner(k, h, dy, cols):
        slot, device = (3 - dy) // 2, (fs, at_y(dy, cols))
        remote(pb.at[k, h], rbuf.at[slot, c, h], ssem.at[9], rsem.at[slot, c, h], device).start()

    def hand_on(k, h, cols, role):
        dy = 1 - 2 * h

        @pl.when(role == 2)
        def _():
            for p in PIECES:
                there, sem = relay_in.at[h, cols, p], relsem.at[h, cols, p]
                remote(pb.at[k, h, p], there, ssem.at[9], sem, (fs, at_y(dy, c))).start()

        @pl.when(role == 3 - 2 * h)
        def _():
            to_owner(k, h, -dy, cols)

        @pl.when((role == 0) & (cols == c))
        def _():
            rbuf[0, c, h] = pb[k, h]

        @pl.when((role == 0) & (cols != c))
        def _():
            remote(pb.at[k, h], rbuf.at[0, c, h], ssem.at[9], rsem.at[0, c, h], partner).start()

    def part_of(core, k):
        block = concat([dn[core, 2 * k], dn[core, 2 * k + 1]], 1)
        return jnp.dot(hid[core], block, preferred_element_type=f32)

    def own_part(dz, other, at):
        k, cols, role = pair_of(dz, other)
        early[at] = part_of(c, k)

    def columns_done(k, cols, role, total):
        for h in range(2):
            for p in PIECES:
                pb[k, h, p] = total[LEN * p : LEN * p + LEN, 128 * h : 128 * h + 128].astype(bf16)
        for h in range(2):
            hand_on(k, h, cols, role)

    def owner_columns(dz, other):
        k, cols, role = pair_of(dz, other)
        columns_done(k, cols, role, part_of(c, k) + part_of(1 - c, k))

    def owner_rest(dz, other, at):
        k, cols, role = pair_of(dz, other)
        columns_done(k, cols, role, early[at] + part_of(1 - c, k))

    def part_at(core, steps):
        block = concat([dn[core, at_fs(dx, dz)] for dx, dz in steps], 1)
        return jnp.dot(hid[core], block, preferred_element_type=f32)

    def halves_done(steps, total):
        for i, (dx, dz) in enumerate(steps):
            j = at_fs(dx, dz)
            k, h = j // 2, j % 2
            for p in PIECES:
                part = total[LEN * p : LEN * p + LEN, 128 * i : 128 * i + 128]
                pb[k, h, p] = part.astype(bf16)
            hand_on(k, h, k % 2, (k // 2 - y + 4) % 4)

    def owner_halves(steps):
        halves_done(steps, part_at(c, steps) + part_at(1 - c, steps))

    def own_halves(steps, at):
        early[at, :, 0 : 128 * len(steps)] = part_at(c, steps)

    def rest_halves(steps, at):
        halves_done(steps, early[at, :, 0 : 128 * len(steps)] + part_at(1 - c, steps))

    def add_half(k, h):
        cols, role = k % 2, (k // 2 - y + 4) % 4

        @pl.when(role == 1 + 2 * h)
        def _():
            for p in PIECES:
                got(relay_in.at[h, cols, p], relsem.at[h, cols, p])
                total = pb[k, h, p].astype(f32) + relay_in[h, cols, p].astype(f32)
                pb[k, h, p] = total.astype(bf16)
                dy = 1 - 2 * h
                there, sem = rbuf.at[(3 - dy) // 2, c, h, p], rsem.at[(3 - dy) // 2, c, h]
                remote(pb.at[k, h, p], there, ssem.at[9], sem, (fs, at_y(dy, cols))).start()

    def half_added(dx, dz):
        j = at_fs(dx, dz)
        add_half(j // 2, j % 2)

    def owner_added(dz, other):
        k, cols, role = pair_of(dz, other)
        for h in range(2):
            add_half(k, h)

    mate = 1 - 2 * (x % 2)
    across_wait(dn, dd, 0)
    owner_columns(0, 0)
    down.run((0, 2, True, []))
    down.run((-1, 1, True, [UP]))
    across_wait(dn, dd, 1)
    owner_columns(0, 1)
    down.run((2, 1, True, [UP]))
    owner_halves([(0, 2)])
    down.run((1, -1, True, []), (-1, -1, True, []))
    own_part(1, 0, 0)
    own_part(-1, 0, 1)
    own_halves([(-mate, 1), (-mate, -1)], 2)
    owner_added(0, 0)
    across_wait(dn, dd, 2)
    owner_rest(1, 0, 0)
    owner_rest(-1, 0, 1)
    rest_halves([(-mate, 1), (-mate, -1)], 2)
    down.run((2, -1, True, []), (1, 2, True, []), (-1, 2, True, []))
    own_halves([(mate, 2), (-mate, 2)], 0)
    own_halves([(2, 1), (2, -1)], 1)
    owner_added(0, 1)
    half_added(0, 2)
    across_wait(dn, dd, 3)
    rest_halves([(mate, 2), (-mate, 2)], 0)
    down.run((2, 2, True, []))
    rest_halves([(2, 1), (2, -1)], 1)
    own_halves([(2, 2)], 0)
    across_wait(dn, dd, 4)
    rest_halves([(2, 2)], 0)
    owner_added(1, 0)
    owner_added(-1, 0)
    half_added(-mate, 1)
    half_added(-mate, -1)
    half_added(mate, 2)
    half_added(-mate, 2)
    half_added(2, 1)
    half_added(2, -1)
    half_added(2, 2)

    for slot in (1, 2):
        for core in range(2):
            for h in range(2):
                    got(rbuf.at[slot, core, h], rsem.at[slot, core, h])
    for h in range(2):
        got(rbuf.at[0, 1 - c, h], rsem.at[0, 1 - c, h])
    for core in range(2):
        for h in range(2):
            total = sum(rbuf[slot, core, h].reshape(TOK, 128).astype(f32) for slot in range(3))
            out[TOK * core : TOK * core + TOK, 128 * h : 128 * h + 128] = total.astype(bf16)

    for ref, i in (
        (pw.at[0, 0:15], 0), (gu.at[0, 0:15], 1), (dn.at[0, 0:15], 2), (xs.at[0:3], 3), (sv, 4),
        (gu.at[0], 5), (dn.at[0], 6), (pw.at[0:4], 7), (pw.at[0:3], 8), (pb.at[0:7], 9),
    ):
        got(ref, ssem.at[i])


def body(
    stream, gain_mix, pool_weight, pool_gain, gain_ffn, gate_weight, up_weight, gate_taps, up_taps,
    down_weight,
):
    row = lambda v: v.reshape(1, 2048)
    DMA = pltpu.SemaphoreType.DMA
    return pl.pallas_call(
        kernel,
        name="layer",
        out_shape=jax.ShapeDtypeStruct((512, 256), bf16),
        in_specs=[pl.BlockSpec(memory_space=pltpu.HBM)] * 10,
        out_specs=pl.BlockSpec(memory_space=pltpu.VMEM),
        scratch_shapes=[
            pltpu.VMEM((2, 16, 1408, 128), bf16),
            pltpu.VMEM((2, 16, 704, 128), bf16),
            pltpu.VMEM((8, 16, 64, 128), bf16),
            pltpu.VMEM((4, 2, TOK, 256), bf16),
            pltpu.VMEM((TOK, 256), bf16),
            pltpu.VMEM((4, 32, 64), bf16),
            pltpu.VMEM((3, 1, 2048), f32),
            pltpu.VMEM((2, 3, 1408), f32),
            pltpu.VMEM((2, 2, 3, 704), f32),
            pltpu.VMEM((512, 512), bf16),
            pltpu.VMEM((512, 512), bf16),
            pltpu.VMEM((4, LEN, LEN), bf16),
            pltpu.VMEM((4, 8, 512), f32),
            pltpu.VMEM((4, TOK, 512), bf16),
            pltpu.VMEM((4, 512, 512), bf16),
            pltpu.VMEM((16, TOK, 128), bf16),
            pltpu.VMEM((TOK, 128), f32),
            pltpu.VMEM((2, TOK, 704), bf16),
            pltpu.VMEM((8, 2, 2, LEN, 128), bf16),
            pltpu.VMEM((3, 2, 2, 2, LEN, 128), bf16),
            pltpu.VMEM((2, 2, TOK, 704), f32),
            pltpu.VMEM((2, 2, 2, LEN, 128), bf16),
            pltpu.VMEM((4, TOK, 256), f32),
            DMA((11,)),
            DMA((16,)),
            DMA((16,)),
            DMA((2,)),
            DMA((5,)),
            DMA((5,)),
            DMA((6,)),
            DMA((4,)),
            DMA((2, 3)),
            DMA((1,)),
            DMA((3, 2, 2)),
            DMA((10,)),
            DMA((2, 2, 2)),
        ],
        compiler_params=pltpu.CompilerParams(
            collective_id=0, has_side_effects=True, vmem_limit_bytes=50 * 1024 * 1024
        ),
    )(
        *[pltpu.with_memory_space_constraint(v, pltpu.HBM) for v in (
        stream, row(gain_mix), pool_weight, row(pool_gain), row(gain_ffn), gate_weight.T, up_weight.T,
        gate_taps, up_taps, down_weight)]
    )


def solution(mesh):
    return jax.shard_map(
        body,
        mesh=mesh,
        in_specs=(
            P("fs", "tp"), P(), P(None, "fs", "tp"), P(), P(), P("fs", "tp"), P("fs", "tp"), P(), P(),
            P("tp", "fs"),
        ),
        out_specs=P("fs", "tp"),
        check_vma=False,
    )
```

```python
import jax
import jax.numpy as jnp
from jax import lax
from jax.experimental import pallas as pl
from jax.experimental.pallas import tpu as pltpu
from jax.sharding import PartitionSpec as P

MESH = pl.DeviceIdType.MESH
bf16, f32 = jnp.bfloat16, jnp.float32
EPS = 1e-6
LEN = 128
PIECES = (0, 1)
TOK = 256


def concat(parts, axis):
    return jnp.concatenate(parts, axis=axis)


def iota(shape, dim):
    return lax.broadcasted_iota(jnp.int32, shape, dim)


def kernel(
    stream, gain_mix, pool_weight, pool_gain, gain_ffn, gate_weight, up_weight, gate_taps, up_taps,
    down_weight,
    out,
    gu, dn, pw, xs, sv, pv, gv, tv, taps, perm, unperm, band, gains, xg, wg, nf, acc, hid,
    pb, rbuf, sums, relay_in, early,
    lsem, gsem, dsem, psem, gd, dd, pys, pds, xys, xds, rsem, ssem, relsem,
):
    fs, tp = lax.axis_index("fs"), lax.axis_index("tp")
    z, x = fs // 4, fs % 4
    y, c = tp // 2, tp % 2

    def at_fs(dx, dz):
        return ((z + dz + 4) % 4) * 4 + (x + dx + 4) % 4

    def at_y(dy, core):
        return ((y + dy + 4) % 4) * 2 + core

    partner = (fs, y * 2 + (1 - c))

    barrier = pltpu.get_barrier_semaphore()
    near = [(dx, dz) for dz in (0, 1, -1) for dx in (0, 1, -1)][1:]
    peers = [(at_fs(dx, dz), tp) for dx, dz in near]
    peers += [(fs, at_y(dy, core)) for dy in (1, -1) for core in (0, 1)] + [partner]
    for peer in peers:
        pl.semaphore_signal(barrier, inc=1, device_id=peer, device_id_type=MESH)

    loads = [
        (pool_weight, pv),
        (gate_weight, gu.at[c, fs, pl.ds(0, 704)]),
        (up_weight, gu.at[c, fs, pl.ds(704, 704)]),
        (stream.at[pl.ds(pl.multiple_of(c * TOK, TOK), TOK)], xs.at[y, c]),
        (stream.at[pl.ds(pl.multiple_of((1 - c) * TOK, TOK), TOK)], sv),
        (down_weight, dn.at[c, fs]),
        (gain_mix, gv.at[0]),
        (pool_gain, gv.at[1]),
        (gain_ffn, gv.at[2]),
        (gate_taps.at[:, pl.ds(pl.multiple_of(y * 1408, 128), 1408)], tv.at[0]),
        (up_taps.at[:, pl.ds(pl.multiple_of(y * 1408, 128), 1408)], tv.at[1]),
    ]
    loads = [pltpu.make_async_copy(a, b, lsem.at[i]) for i, (a, b) in enumerate(loads)]
    for load in loads:
        load.start()
    loads[0].wait()
    for p in range(2):
        pw[tp, fs, 32 * p : 32 * p + 32, :] = concat([pv[2 * p], pv[2 * p + 1]], 1)
    for load in loads[1:5]:
        load.wait()
    pl.semaphore_wait(barrier, len(peers))

    def remote(src, dst, send, recv, device):
        return pltpu.make_async_remote_copy(
            src_ref=src, dst_ref=dst, send_sem=send, recv_sem=recv, device_id=device,
            device_id_type=MESH,
        )

    def got(ref, sem):
        pltpu.make_async_copy(ref, ref, sem).wait()

    def group(a, b):
        return {0: 0, 1: 0, 4: 1, 2: 2, 5: 3, 8: 4}[a * a + b * b]

    class Tree:
        def __init__(self, block, rows, recv, send, cross, cross_send):
            self.block, self.rows, self.recv, self.send = block, rows, recv, send
            self.cross, self.cross_send = cross, cross_send

        def ref(self, q, a, b):
            color, sign = q // 2, 1 - 2 * (q % 2)
            j = at_fs(-sign * (a * (1 - color) + b * color), -sign * (a * color + b * (1 - color)))
            rows = pl.ds(pl.multiple_of(q * self.rows, self.rows), self.rows)
            return self.block(j).at[rows]

        def push(self, q, a, b, da, db):
            color, sign = q // 2, 1 - 2 * (q % 2)
            to = at_fs(sign * (da * (1 - color) + db * color), sign * (da * color + db * (1 - color)))
            ref = self.ref(q, a, b)
            pos = ((a + da) % 4) * 4 + (b + db) % 4
            remote(ref, ref, self.send, self.recv.at[pos], (to, tp)).start()

        def await_(self, a, b):
            ref = self.block(fs)
            pltpu.make_async_copy(ref, ref, self.recv.at[(a % 4) * 4 + b % 4]).wait()

        def each(self, f):
            def go(q, carry):
                f(q)
                return carry

            lax.fori_loop(0, 4, go, 0)

        def run(self, *items):
            for a, b, wait, steps in items:
                if wait:
                    self.await_(a, b)

                def f(q):
                    for da, db in steps:
                        self.push(q, a, b, da, db)
                    if wait:
                        ref = self.ref(q, a, b)
                        sem = self.cross.at[group(a, b)]
                        remote(ref, ref, self.cross_send, sem, partner).start()

                self.each(f)

    gup = Tree(lambda j: gu.at[c, j], 352, gsem, ssem.at[1], gd, ssem.at[5])
    down = Tree(lambda j: dn.at[c, j], 176, dsem, ssem.at[2], dd, ssem.at[6])

    def across(blocks, recv, send):
        remote(blocks.at[c, fs], blocks.at[c, fs], send, recv.at[0], partner).start()

    def across_wait(blocks, recv, i):
        count = (5, 2, 4, 4, 1)[i]
        got(blocks.at[1 - c, 0:count], recv.at[i])

    NEAR = [(1, 0), (-1, 0), (0, 1), (0, -1)]
    FAR = [(2, 0), (0, 2)]
    DIAG = [(1, 1), (1, -1), (-1, 1), (-1, -1)]
    KNIGHT = [(2, 1), (2, -1), (1, 2), (-1, 2)]

    def piece(dy, p):
        return xs.at[(y + dy + 4) % 4, p]

    def piece_out(p):
        remote(piece(0, p), piece(0, p), ssem.at[3], xys.at[p, 0], (fs, at_y(1, c))).start()
        remote(piece(0, p), piece(0, p), ssem.at[3], xys.at[p, 1], (fs, at_y(-1, c))).start()

    RIGHT, LEFT, UP, DOWN = (1, 0), (-1, 0), (0, 1), (0, -1)
    remote(sv, xs.at[y, c], ssem.at[4], xds.at[0], partner).start()
    piece_out(c)
    for dx, dz in near:
        mine = pw.at[tp, fs]
        remote(mine, mine, ssem.at[0], psem.at[0], (at_fs(dx, dz), tp)).start()
    gup.run((0, 0, False, [RIGHT]))
    gup.run((0, 0, False, [UP]))
    gup.run((0, 0, False, [LEFT]))
    across(gu, gd, ssem.at[5])
    for load in loads[5:]:
        load.wait()
    across(dn, dd, ssem.at[6])

    d, n = iota((512, 512), 0), iota((512, 512), 1)
    perm[...] = ((d % 4) * 128 + d // 4 == n).astype(bf16)
    unperm[...] = ((n % 4) * 128 + n // 4 == d).astype(bf16)
    row, col = iota((LEN, LEN), 0), iota((LEN, LEN), 1)
    for g in range(4):
        band[g] = ((col <= row) & (col > row - 2 ** (g + 1))).astype(bf16)

    got(xs.at[y, 1 - c], xds.at[0])
    piece_out(1 - c)

    three = concat([gv[0], gv[1], gv[2], jnp.zeros((5, 2048), f32)], 0)
    high = three.astype(bf16)
    rest = three - high.astype(f32)
    mid = rest.astype(bf16)
    low = (rest - mid.astype(f32)).astype(bf16)
    for yy in range(4):
        s = slice(512 * yy, 512 * yy + 512)
        moved = sum(jnp.dot(v[:, s], perm[...], preferred_element_type=f32) for v in (low, mid, high))
        for g in range(4):
            gains[g, :, 128 * yy : 128 * yy + 128] = moved[:, 128 * g : 128 * g + 128]
    for core in range(2):
        a = 704 * core
        taps[core, 0] = tv[0, :, a : a + 704]
        taps[core, 1] = tv[1, :, a : a + 704]

    got(pw.at[tp, 0:8], psem.at[0])

    def onward(ox, oz, half, dx, dz):
        ref = pw.at[tp, at_fs(ox, oz), pl.ds(32 * half, 32)]
        remote(ref, ref, ssem.at[0], psem.at[1], (at_fs(dx, dz), tp)).start()

    for o in (0, 1, -1):
        onward(-1, o, 0, 1, 0)
        onward(1, o, 1, -1, 0)
        onward(o, -1, 0, 0, 1)
        onward(o, 1, 1, 0, -1)
    onward(-1, -1, 0, 1, 1)
    onward(1, 1, 1, -1, -1)
    gup.run((1, 0, True, [RIGHT]))
    gup.run((0, 0, False, [DOWN]))
    gup.run((1, 0, False, [UP]))
    got(piece(-1, 0), xys.at[0, 0])
    remote(piece(-1, 0), piece(-1, 0), ssem.at[3], xys.at[0, 2], (fs, at_y(1, c))).start()
    got(piece(1, 1), xys.at[1, 1])
    remote(piece(1, 1), piece(1, 1), ssem.at[3], xys.at[1, 2], (fs, at_y(-1, c))).start()
    got(pw.at[tp, 0:7], psem.at[1])

    def columns(dy, core):
        return pw.at[at_y(dy, core)]

    def pool_across(i, dy):
        remote(columns(dy, c), columns(dy, c), ssem.at[7], pds.at[i], partner).start()

    def half_out(dy, half, sem, to):
        ref = columns(dy, c).at[pl.ds(8 * half, 8)]
        remote(ref, ref, ssem.at[8], pys.at[sem], (fs, at_y(to, c))).start()

    def half_in(dy, half, sem):
        got(columns(dy, c).at[pl.ds(8 * half, 8)], pys.at[sem])

    half_out(0, 0, 0, 1)
    half_out(0, 1, 2, -1)
    half_out(0, 1, 1, 1)
    half_out(0, 0, 3, -1)
    pool_across(0, 0)
    gup.run((2, 0, True, [UP]))
    gup.run((-1, 0, True, [UP]))
    gup.run((0, 1, True, [UP]), (1, 0, False, [DOWN]), (2, 0, False, [DOWN]), (-1, 0, False, [DOWN]))

    acc[...] = jnp.zeros_like(acc)

    def regroup(yy, carry):
        xp = jnp.dot(concat([xs[yy, 0], xs[yy, 1]], 1), perm[...], preferred_element_type=f32)
        at = pl.ds(pl.multiple_of(yy * 128, 128), 128)
        total = acc[...]
        for g in range(4):
            part = xp[:, 128 * g : 128 * g + 128]
            xg[g, :, at] = part.astype(bf16)
            total = total + part * part
        acc[...] = total
        return carry

    def unpack(yy, carry):
        at = pl.ds(pl.multiple_of(yy * 128, 128), 128)
        for p in range(2):
            left = pw[2 * yy, :, 32 * p : 32 * p + 32, :].reshape(512, 128)
            right = pw[2 * yy + 1, :, 32 * p : 32 * p + 32, :].reshape(512, 128)
            wg[2 * p, :, at] = concat([left[:, 0:64], right[:, 0:64]], 1)
            wg[2 * p + 1, :, at] = concat([left[:, 64:128], right[:, 64:128]], 1)
        return carry

    got(piece(1, 0), xys.at[0, 1])
    got(piece(-1, 1), xys.at[1, 0])
    regroup(y, 0)
    regroup((y + 1) % 4, 0)
    regroup((y + 3) % 4, 0)
    gup.run((0, -1, True, []))
    gup.run((1, 1, True, [UP]))
    down.run((0, 0, False, [RIGHT]))
    got(columns(0, 1 - c), pds.at[0])
    unpack(y, 0)
    half_in(-1, 0, 0)
    half_out(-1, 0, 4, 1)
    half_in(1, 1, 2)
    half_out(1, 1, 5, -1)
    gup.run((2, 1, True, [UP]))
    got(piece(2, 0), xys.at[0, 2])
    got(piece(2, 1), xys.at[1, 2])
    regroup((y + 2) % 4, 0)
    gup.run((-1, 1, True, [UP]))
    down.run((0, 0, False, [UP]))
    down.run((0, 0, False, [LEFT]))
    down.run((0, 0, False, [DOWN]))
    half_in(-1, 1, 1)
    pool_across(1, -1)
    half_in(1, 0, 3)
    pool_across(2, 1)
    got(columns(-1, 1 - c), pds.at[1])
    unpack((y + 3) % 4, 0)
    got(columns(1, 1 - c), pds.at[2])
    unpack((y + 1) % 4, 0)
    half_in(2, 0, 4)
    half_in(2, 1, 5)
    pool_across(3, 2)
    gup.run((0, 2, True, []))
    got(columns(2, 1 - c), pds.at[3])
    unpack((y + 2) % 4, 0)

    scale = lax.rsqrt(jnp.sum(acc[...], axis=1, keepdims=True) * (1.0 / 2048) + EPS)
    acc[...] = jnp.zeros_like(acc)
    position = iota((LEN, 512), 0) + 1

    def mix(g, carry):
        divisor = jnp.minimum(position, lax.shift_left(2, g)).astype(f32)
        normed = (xg[g].astype(f32) * scale * gains[g, 0:1, :]).astype(bf16)
        pooled = []
        for s in range(TOK // LEN):
            part = normed[LEN * s : LEN * s + LEN]
            window = jnp.dot(band[g], part, preferred_element_type=f32)
            pooled.append((window / divisor - part.astype(f32)).astype(bf16))
        mixer = jnp.dot(concat(pooled, 0), wg[g], preferred_element_type=f32) * gains[g, 1:2, :]
        middle = (xg[g].astype(f32) + mixer).astype(bf16)
        xg[g] = middle
        total = acc[...]
        for i in range(4):
            part = middle[:, 128 * i : 128 * i + 128].astype(f32)
            total = total + part * part
        acc[...] = total
        return carry

    lax.fori_loop(0, 4, mix, 0)
    scale = lax.rsqrt(jnp.sum(acc[...], axis=1, keepdims=True) * (1.0 / 2048) + EPS)

    def rescale(g, carry):
        xg[g] = (xg[g].astype(f32) * scale * gains[g, 2:3, :]).astype(bf16)
        return carry

    lax.fori_loop(0, 4, rescale, 0)

    def natural(yy, carry):
        at = pl.ds(pl.multiple_of(yy * 128, 128), 128)
        grouped = concat([xg[g, :, at] for g in range(4)], 1)
        moved = jnp.dot(grouped, unperm[...], preferred_element_type=f32).astype(bf16)
        for i in range(4):
            nf[4 * yy + i] = moved[:, 128 * i : 128 * i + 128]
        return carry

    lax.fori_loop(0, 4, natural, 0)

    SETS = ([(0, 0)] + NEAR, FAR + DIAG, KNIGHT + [(2, 2)])
    CHUNKS = ((0, 256), (256, 256), (512, 192))

    def product(core, which, at, width, offsets):
        js = [at_fs(dx, dz) for dx, dz in offsets]
        left = concat([nf[j] for j in js], 1)
        right = concat([gu[core, j, pl.ds(704 * which + at, width), :] for j in js], 1)
        return lax.dot_general(left, right, (((1,), (1,)), ((), ())), preferred_element_type=f32)

    def gather_up(core, i):
        for which in range(2):
            for at, width in CHUNKS:
                part = product(core, which, at, width, SETS[i])
                if i > 0:
                    part = sums[core, which, :, at : at + width] + part
                sums[core, which, :, at : at + width] = part

    def conv(core, which, at, width):
        v = sums[core, which, :, at : at + width] + product(core, which, at, width, SETS[2])
        v = v.astype(bf16).astype(f32)
        k = taps[core, which, :, at : at + width]
        place = iota((TOK, width), 0) % LEN
        back1 = jnp.where(place >= 1, pltpu.roll(v, 1, 0), 0.0)
        back2 = jnp.where(place >= 2, pltpu.roll(v, 2, 0), 0.0)
        return back2 * k[0:1] + back1 * k[1:2] + v * k[2:3]

    def units(core, t):
        at, width = CHUNKS[t]
        a, b = conv(core, 0, at, width), conv(core, 1, at, width)
        hid[core, :, at : at + width] = (a / (1.0 + jnp.exp(-a)) * b).astype(bf16)

    gather_up(c, 0)
    across_wait(gu, gd, 0)
    gather_up(1 - c, 0)
    gup.run((1, -1, True, []), (-1, -1, True, []), (2, -1, True, []))
    gather_up(c, 1)
    down.run((1, 0, True, [RIGHT, UP]))
    across_wait(gu, gd, 1)
    across_wait(gu, gd, 2)
    gather_up(1 - c, 1)
    gup.run((1, 2, True, []), (2, 2, True, []), (-1, 2, True, []))
    units(c, 0)
    down.run((0, 1, True, [UP]))
    units(c, 1)
    down.run((-1, 0, True, [UP, DOWN]), (1, 0, False, [DOWN]))
    units(c, 2)
    across_wait(gu, gd, 3)
    across_wait(gu, gd, 4)
    units(1 - c, 0)
    down.run((0, -1, True, []))
    units(1 - c, 1)
    down.run((2, 0, True, [UP, DOWN]))
    units(1 - c, 2)
    down.run((1, 1, True, [UP]))

    def pair_of(dz, other):
        cols = x // 2 if other == 0 else 1 - x // 2
        zk = (z + dz + 4) % 4
        return zk * 2 + cols, cols, (zk - y + 4) % 4

    def to_owner(k, h, dy, cols):
        slot, device = (3 - dy) // 2, (fs, at_y(dy, cols))
        remote(pb.at[k, h], rbuf.at[slot, c, h], ssem.at[9], rsem.at[slot, c, h], device).start()

    def hand_far(k, h, cols, role):
        dy = 1 - 2 * h

        @pl.when(role == 2)
        def _():
            for p in PIECES:
                there, sem = relay_in.at[h, cols, p], relsem.at[h, cols, p]
                remote(pb.at[k, h, p], there, ssem.at[9], sem, (fs, at_y(dy, c))).start()

    def hand_near(k, h, cols, role):
        dy = 1 - 2 * h

        @pl.when(role == 3 - 2 * h)
        def _():
            to_owner(k, h, -dy, cols)

        @pl.when((role == 0) & (cols == c))
        def _():
            rbuf[0, c, h] = pb[k, h]

        @pl.when((role == 0) & (cols != c))
        def _():
            remote(pb.at[k, h], rbuf.at[0, c, h], ssem.at[9], rsem.at[0, c, h], partner).start()

    def part_of(core, k):
        block = concat([dn[core, 2 * k], dn[core, 2 * k + 1]], 1)
        return jnp.dot(hid[core], block, preferred_element_type=f32)

    def own_part(dz, other, at):
        k, cols, role = pair_of(dz, other)
        early[at] = part_of(c, k)

    def columns_done(k, cols, role, total):
        for h in range(2):
            for p in PIECES:
                pb[k, h, p] = total[LEN * p : LEN * p + LEN, 128 * h : 128 * h + 128].astype(bf16)
        for h in range(2):
            hand_far(k, h, cols, role)
        for h in range(2):
            hand_near(k, h, cols, role)

    def owner_columns(dz, other):
        k, cols, role = pair_of(dz, other)
        columns_done(k, cols, role, part_of(c, k) + part_of(1 - c, k))

    def owner_rest(dz, other, at):
        k, cols, role = pair_of(dz, other)
        columns_done(k, cols, role, early[at] + part_of(1 - c, k))

    def part_at(core, steps):
        block = concat([dn[core, at_fs(dx, dz)] for dx, dz in steps], 1)
        return jnp.dot(hid[core], block, preferred_element_type=f32)

    def halves_done(steps, total, near=True):
        for i, (dx, dz) in enumerate(steps):
            j = at_fs(dx, dz)
            k, h = j // 2, j % 2
            for p in PIECES:
                part = total[LEN * p : LEN * p + LEN, 128 * i : 128 * i + 128]
                pb[k, h, p] = part.astype(bf16)
            hand_far(k, h, k % 2, (k // 2 - y + 4) % 4)
        if near:
            near_done(steps)

    def near_done(steps):
        for dx, dz in steps:
            j = at_fs(dx, dz)
            k, h = j // 2, j % 2
            hand_near(k, h, k % 2, (k // 2 - y + 4) % 4)

    def owner_halves(steps):
        halves_done(steps, part_at(c, steps) + part_at(1 - c, steps))

    def own_halves(steps, at):
        early[at, :, 0 : 128 * len(steps)] = part_at(c, steps)

    def rest_halves(steps, at, near=True):
        halves_done(steps, early[at, :, 0 : 128 * len(steps)] + part_at(1 - c, steps), near)

    def add_half(k, h):
        cols, role = k % 2, (k // 2 - y + 4) % 4

        @pl.when(role == 1 + 2 * h)
        def _():
            for p in PIECES:
                got(relay_in.at[h, cols, p], relsem.at[h, cols, p])
                total = pb[k, h, p].astype(f32) + relay_in[h, cols, p].astype(f32)
                pb[k, h, p] = total.astype(bf16)
                dy = 1 - 2 * h
                there, sem = rbuf.at[(3 - dy) // 2, c, h, p], rsem.at[(3 - dy) // 2, c, h]
                remote(pb.at[k, h, p], there, ssem.at[9], sem, (fs, at_y(dy, cols))).start()

    def half_added(dx, dz):
        j = at_fs(dx, dz)
        add_half(j // 2, j % 2)

    def owner_added(dz, other):
        k, cols, role = pair_of(dz, other)
        for h in range(2):
            add_half(k, h)

    mate = 1 - 2 * (x % 2)
    across_wait(dn, dd, 0)
    owner_columns(0, 0)
    down.run((0, 2, True, []))
    down.run((-1, 1, True, [UP]))
    across_wait(dn, dd, 1)
    owner_columns(0, 1)
    owner_halves([(0, 2)])
    down.run((1, -1, True, []), (-1, -1, True, []))
    own_part(1, 0, 0)
    own_part(-1, 0, 1)
    own_halves([(-mate, 1), (-mate, -1)], 2)
    across_wait(dn, dd, 2)
    owner_rest(1, 0, 0)
    down.run((2, 1, True, [UP]))
    owner_rest(-1, 0, 1)
    rest_halves([(-mate, 1), (-mate, -1)], 2)
    owner_added(0, 0)
    down.run((2, -1, True, []))
    down.run((1, 2, True, []))
    down.run((-1, 2, True, []))
    own_halves([(mate, 2), (-mate, 2)], 0)
    own_halves([(2, 1), (2, -1)], 1)
    owner_added(0, 1)
    half_added(0, 2)
    across_wait(dn, dd, 3)
    rest_halves([(mate, 2), (-mate, 2)], 0, False)
    rest_halves([(2, 1), (2, -1)], 1)
    near_done([(mate, 2), (-mate, 2)])
    down.run((2, 2, True, []))
    own_halves([(2, 2)], 0)
    across_wait(dn, dd, 4)
    rest_halves([(2, 2)], 0)
    owner_added(1, 0)
    owner_added(-1, 0)
    half_added(-mate, 1)
    half_added(-mate, -1)
    half_added(mate, 2)
    half_added(-mate, 2)
    half_added(2, 1)
    half_added(2, -1)
    half_added(2, 2)

    for slot in (1, 2):
        for core in range(2):
            for h in range(2):
                    got(rbuf.at[slot, core, h], rsem.at[slot, core, h])
    for h in range(2):
        got(rbuf.at[0, 1 - c, h], rsem.at[0, 1 - c, h])
    for core in range(2):
        for h in range(2):
            total = sum(rbuf[slot, core, h].reshape(TOK, 128).astype(f32) for slot in range(3))
            out[TOK * core : TOK * core + TOK, 128 * h : 128 * h + 128] = total.astype(bf16)

    for ref, i in (
        (pw.at[0, 0:15], 0), (gu.at[0, 0:15], 1), (dn.at[0, 0:15], 2), (xs.at[0:3], 3), (sv, 4),
        (gu.at[0], 5), (dn.at[0], 6), (pw.at[0:4], 7), (pw.at[0:3], 8), (pb.at[0:7], 9),
    ):
        got(ref, ssem.at[i])


def body(
    stream, gain_mix, pool_weight, pool_gain, gain_ffn, gate_weight, up_weight, gate_taps, up_taps,
    down_weight,
):
    row = lambda v: v.reshape(1, 2048)
    DMA = pltpu.SemaphoreType.DMA
    return pl.pallas_call(
        kernel,
        name="layer",
        out_shape=jax.ShapeDtypeStruct((512, 256), bf16),
        in_specs=[pl.BlockSpec(memory_space=pltpu.HBM)] * 10,
        out_specs=pl.BlockSpec(memory_space=pltpu.VMEM),
        scratch_shapes=[
            pltpu.VMEM((2, 16, 1408, 128), bf16),
            pltpu.VMEM((2, 16, 704, 128), bf16),
            pltpu.VMEM((8, 16, 64, 128), bf16),
            pltpu.VMEM((4, 2, TOK, 256), bf16),
            pltpu.VMEM((TOK, 256), bf16),
            pltpu.VMEM((4, 32, 64), bf16),
            pltpu.VMEM((3, 1, 2048), f32),
            pltpu.VMEM((2, 3, 1408), f32),
            pltpu.VMEM((2, 2, 3, 704), f32),
            pltpu.VMEM((512, 512), bf16),
            pltpu.VMEM((512, 512), bf16),
            pltpu.VMEM((4, LEN, LEN), bf16),
            pltpu.VMEM((4, 8, 512), f32),
            pltpu.VMEM((4, TOK, 512), bf16),
            pltpu.VMEM((4, 512, 512), bf16),
            pltpu.VMEM((16, TOK, 128), bf16),
            pltpu.VMEM((TOK, 128), f32),
            pltpu.VMEM((2, TOK, 704), bf16),
            pltpu.VMEM((8, 2, 2, LEN, 128), bf16),
            pltpu.VMEM((3, 2, 2, 2, LEN, 128), bf16),
            pltpu.VMEM((2, 2, TOK, 704), f32),
            pltpu.VMEM((2, 2, 2, LEN, 128), bf16),
            pltpu.VMEM((4, TOK, 256), f32),
            DMA((11,)),
            DMA((16,)),
            DMA((16,)),
            DMA((2,)),
            DMA((5,)),
            DMA((5,)),
            DMA((6,)),
            DMA((4,)),
            DMA((2, 3)),
            DMA((1,)),
            DMA((3, 2, 2)),
            DMA((10,)),
            DMA((2, 2, 2)),
        ],
        compiler_params=pltpu.CompilerParams(
            collective_id=0, has_side_effects=True, vmem_limit_bytes=50 * 1024 * 1024
        ),
    )(
        *[pltpu.with_memory_space_constraint(v, pltpu.HBM) for v in (
        stream, row(gain_mix), pool_weight, row(pool_gain), row(gain_ffn), gate_weight.T, up_weight.T,
        gate_taps, up_taps, down_weight)]
    )


def solution(mesh):
    return jax.shard_map(
        body,
        mesh=mesh,
        in_specs=(
            P("fs", "tp"), P(), P(None, "fs", "tp"), P(), P(), P("fs", "tp"), P("fs", "tp"), P(), P(),
            P("tp", "fs"),
        ),
        out_specs=P("fs", "tp"),
        check_vma=False,
    )
```

```python
import jax
import jax.numpy as jnp
from jax import lax
from jax.experimental import pallas as pl
from jax.experimental.pallas import tpu as pltpu
from jax.sharding import PartitionSpec as P

MESH = pl.DeviceIdType.MESH
bf16, f32 = jnp.bfloat16, jnp.float32
EPS = 1e-6
LEN = 128
PIECES = (0, 1)
TOK = 256


def concat(parts, axis):
    return jnp.concatenate(parts, axis=axis)


def iota(shape, dim):
    return lax.broadcasted_iota(jnp.int32, shape, dim)


def kernel(
    stream, gain_mix, pool_weight, pool_gain, gain_ffn, gate_weight, up_weight, gate_taps, up_taps,
    down_weight,
    out,
    gu, dn, pw, xs, sv, pv, gv, tv, taps, perm, unperm, band, gains, xg, wg, nf, acc, hid,
    pb, rbuf, sums, relay_in, early,
    lsem, gsem, dsem, psem, gd, dd, pys, pds, xys, xds, rsem, ssem, relsem, ready,
):
    fs, tp = lax.axis_index("fs"), lax.axis_index("tp")
    z, x = fs // 4, fs % 4
    y, c = tp // 2, tp % 2

    def at_fs(dx, dz):
        return ((z + dz + 4) % 4) * 4 + (x + dx + 4) % 4

    def at_y(dy, core):
        return ((y + dy + 4) % 4) * 2 + core

    partner = (fs, y * 2 + (1 - c))

    barrier = pltpu.get_barrier_semaphore()
    near = [(dx, dz) for dz in (0, 1, -1) for dx in (0, 1, -1)][1:]
    beside = [(at_fs(dx, dz), tp) for dx, dz in near if dx * dz == 0]
    peers = list(beside)
    peers += [(fs, at_y(dy, core)) for dy in (1, -1) for core in (0, 1)] + [partner]
    for peer in peers:
        pl.semaphore_signal(barrier, inc=1, device_id=peer, device_id_type=MESH)

    loads = [
        (pool_weight, pv),
        (gate_weight, gu.at[c, fs, pl.ds(0, 704)]),
        (up_weight, gu.at[c, fs, pl.ds(704, 704)]),
        (stream.at[pl.ds(pl.multiple_of(c * TOK, TOK), TOK)], xs.at[y, c]),
        (stream.at[pl.ds(pl.multiple_of((1 - c) * TOK, TOK), TOK)], sv),
        (down_weight, dn.at[c, fs]),
        (gain_mix, gv.at[0]),
        (pool_gain, gv.at[1]),
        (gain_ffn, gv.at[2]),
        (gate_taps.at[:, pl.ds(pl.multiple_of(y * 1408, 128), 1408)], tv.at[0]),
        (up_taps.at[:, pl.ds(pl.multiple_of(y * 1408, 128), 1408)], tv.at[1]),
    ]
    loads = [pltpu.make_async_copy(a, b, lsem.at[i]) for i, (a, b) in enumerate(loads)]
    for load in loads:
        load.start()
    loads[0].wait()
    for p in range(2):
        pw[tp, fs, 32 * p : 32 * p + 32, :] = concat([pv[2 * p], pv[2 * p + 1]], 1)
    for load in loads[1:5]:
        load.wait()
    pl.semaphore_wait(barrier, len(peers))

    def remote(src, dst, send, recv, device):
        return pltpu.make_async_remote_copy(
            src_ref=src, dst_ref=dst, send_sem=send, recv_sem=recv, device_id=device,
            device_id_type=MESH,
        )

    def got(ref, sem):
        pltpu.make_async_copy(ref, ref, sem).wait()

    def group(a, b):
        return {0: 0, 1: 0, 4: 1, 2: 2, 5: 3, 8: 4}[a * a + b * b]

    class Tree:
        def __init__(self, block, rows, recv, send, cross, cross_send):
            self.block, self.rows, self.recv, self.send = block, rows, recv, send
            self.cross, self.cross_send = cross, cross_send

        def ref(self, q, a, b):
            color, sign = q // 2, 1 - 2 * (q % 2)
            j = at_fs(-sign * (a * (1 - color) + b * color), -sign * (a * color + b * (1 - color)))
            rows = pl.ds(pl.multiple_of(q * self.rows, self.rows), self.rows)
            return self.block(j).at[rows]

        def push(self, q, a, b, da, db):
            color, sign = q // 2, 1 - 2 * (q % 2)
            to = at_fs(sign * (da * (1 - color) + db * color), sign * (da * color + db * (1 - color)))
            ref = self.ref(q, a, b)
            pos = ((a + da) % 4) * 4 + (b + db) % 4
            remote(ref, ref, self.send, self.recv.at[pos], (to, tp)).start()

        def await_(self, a, b):
            ref = self.block(fs)
            pltpu.make_async_copy(ref, ref, self.recv.at[(a % 4) * 4 + b % 4]).wait()

        def each(self, f):
            def go(q, carry):
                f(q)
                return carry

            lax.fori_loop(0, 4, go, 0)

        def run(self, *items):
            for a, b, wait, steps in items:
                if wait:
                    self.await_(a, b)

                def f(q):
                    for da, db in steps:
                        self.push(q, a, b, da, db)
                    if wait:
                        ref = self.ref(q, a, b)
                        sem = self.cross.at[group(a, b)]
                        remote(ref, ref, self.cross_send, sem, partner).start()

                self.each(f)

    gup = Tree(lambda j: gu.at[c, j], 352, gsem, ssem.at[1], gd, ssem.at[5])
    down = Tree(lambda j: dn.at[c, j], 176, dsem, ssem.at[2], dd, ssem.at[6])

    def across(blocks, recv, send):
        remote(blocks.at[c, fs], blocks.at[c, fs], send, recv.at[0], partner).start()

    def across_wait(blocks, recv, i):
        count = (5, 2, 4, 4, 1)[i]
        got(blocks.at[1 - c, 0:count], recv.at[i])

    NEAR = [(1, 0), (-1, 0), (0, 1), (0, -1)]
    FAR = [(2, 0), (0, 2)]
    DIAG = [(1, 1), (1, -1), (-1, 1), (-1, -1)]
    KNIGHT = [(2, 1), (2, -1), (1, 2), (-1, 2)]

    def piece(dy, p):
        return xs.at[(y + dy + 4) % 4, p]

    def piece_out(p):
        remote(piece(0, p), piece(0, p), ssem.at[3], xys.at[p, 0], (fs, at_y(1, c))).start()
        remote(piece(0, p), piece(0, p), ssem.at[3], xys.at[p, 1], (fs, at_y(-1, c))).start()

    for peer in beside:
        pl.semaphore_signal(ready, inc=1, device_id=peer, device_id_type=MESH)
    RIGHT, LEFT, UP, DOWN = (1, 0), (-1, 0), (0, 1), (0, -1)
    remote(sv, xs.at[y, c], ssem.at[4], xds.at[0], partner).start()
    piece_out(c)
    gup.run((0, 0, False, [RIGHT]))
    across(gu, gd, ssem.at[5])
    for load in loads[5:]:
        load.wait()
    across(dn, dd, ssem.at[6])

    d, n = iota((512, 512), 0), iota((512, 512), 1)
    perm[...] = ((d % 4) * 128 + d // 4 == n).astype(bf16)
    unperm[...] = ((n % 4) * 128 + n // 4 == d).astype(bf16)
    row, col = iota((LEN, LEN), 0), iota((LEN, LEN), 1)
    for g in range(4):
        band[g] = ((col <= row) & (col > row - 2 ** (g + 1))).astype(bf16)

    got(xs.at[y, 1 - c], xds.at[0])
    piece_out(1 - c)
    pl.semaphore_wait(ready, len(beside))
    for dx, dz in near:
        mine = pw.at[tp, fs]
        remote(mine, mine, ssem.at[0], psem.at[0], (at_fs(dx, dz), tp)).start()
    gup.run((0, 0, False, [UP]))
    gup.run((0, 0, False, [LEFT]))

    three = concat([gv[0], gv[1], gv[2], jnp.zeros((5, 2048), f32)], 0)
    high = three.astype(bf16)
    rest = three - high.astype(f32)
    mid = rest.astype(bf16)
    low = (rest - mid.astype(f32)).astype(bf16)
    for yy in range(4):
        s = slice(512 * yy, 512 * yy + 512)
        moved = sum(jnp.dot(v[:, s], perm[...], preferred_element_type=f32) for v in (low, mid, high))
        for g in range(4):
            gains[g, :, 128 * yy : 128 * yy + 128] = moved[:, 128 * g : 128 * g + 128]
    for core in range(2):
        a = 704 * core
        taps[core, 0] = tv[0, :, a : a + 704]
        taps[core, 1] = tv[1, :, a : a + 704]

    gup.run((1, 0, True, [RIGHT]))
    got(pw.at[tp, 0:8], psem.at[0])

    def onward(ox, oz, half, dx, dz):
        ref = pw.at[tp, at_fs(ox, oz), pl.ds(32 * half, 32)]
        remote(ref, ref, ssem.at[0], psem.at[1], (at_fs(dx, dz), tp)).start()

    for o in (0, 1, -1):
        onward(-1, o, 0, 1, 0)
        onward(1, o, 1, -1, 0)
        onward(o, -1, 0, 0, 1)
        onward(o, 1, 1, 0, -1)
    onward(-1, -1, 0, 1, 1)
    onward(1, 1, 1, -1, -1)
    gup.run((0, 0, False, [DOWN]))
    gup.run((1, 0, False, [UP]))
    got(piece(-1, 0), xys.at[0, 0])
    remote(piece(-1, 0), piece(-1, 0), ssem.at[3], xys.at[0, 2], (fs, at_y(1, c))).start()
    got(piece(1, 1), xys.at[1, 1])
    remote(piece(1, 1), piece(1, 1), ssem.at[3], xys.at[1, 2], (fs, at_y(-1, c))).start()
    gup.run((2, 0, True, [UP]))
    gup.run((-1, 0, True, [UP]))
    got(pw.at[tp, 0:7], psem.at[1])

    def columns(dy, core):
        return pw.at[at_y(dy, core)]

    def pool_across(i, dy):
        remote(columns(dy, c), columns(dy, c), ssem.at[7], pds.at[i], partner).start()

    def half_out(dy, half, sem, to):
        ref = columns(dy, c).at[pl.ds(8 * half, 8)]
        remote(ref, ref, ssem.at[8], pys.at[sem], (fs, at_y(to, c))).start()

    def half_in(dy, half, sem):
        got(columns(dy, c).at[pl.ds(8 * half, 8)], pys.at[sem])

    half_out(0, 0, 0, 1)
    half_out(0, 1, 2, -1)
    half_out(0, 1, 1, 1)
    half_out(0, 0, 3, -1)
    pool_across(0, 0)
    gup.run((0, 1, True, [UP]), (1, 0, False, [DOWN]), (2, 0, False, [DOWN]), (-1, 0, False, [DOWN]))

    acc[...] = jnp.zeros_like(acc)

    def regroup(yy, carry):
        xp = jnp.dot(concat([xs[yy, 0], xs[yy, 1]], 1), perm[...], preferred_element_type=f32)
        at = pl.ds(pl.multiple_of(yy * 128, 128), 128)
        total = acc[...]
        for g in range(4):
            part = xp[:, 128 * g : 128 * g + 128]
            xg[g, :, at] = part.astype(bf16)
            total = total + part * part
        acc[...] = total
        return carry

    def unpack(yy, carry):
        at = pl.ds(pl.multiple_of(yy * 128, 128), 128)
        for p in range(2):
            left = pw[2 * yy, :, 32 * p : 32 * p + 32, :].reshape(512, 128)
            right = pw[2 * yy + 1, :, 32 * p : 32 * p + 32, :].reshape(512, 128)
            wg[2 * p, :, at] = concat([left[:, 0:64], right[:, 0:64]], 1)
            wg[2 * p + 1, :, at] = concat([left[:, 64:128], right[:, 64:128]], 1)
        return carry

    got(piece(1, 0), xys.at[0, 1])
    got(piece(-1, 1), xys.at[1, 0])
    regroup(y, 0)
    regroup((y + 1) % 4, 0)
    regroup((y + 3) % 4, 0)
    gup.run((0, -1, True, []))
    gup.run((1, 1, True, [UP]))
    down.run((0, 0, False, [RIGHT]))
    got(columns(0, 1 - c), pds.at[0])
    unpack(y, 0)
    half_in(-1, 0, 0)
    half_out(-1, 0, 4, 1)
    half_in(1, 1, 2)
    half_out(1, 1, 5, -1)
    gup.run((2, 1, True, [UP]))
    got(piece(2, 0), xys.at[0, 2])
    got(piece(2, 1), xys.at[1, 2])
    regroup((y + 2) % 4, 0)
    gup.run((-1, 1, True, [UP]))
    down.run((0, 0, False, [UP]))
    down.run((0, 0, False, [LEFT]))
    down.run((0, 0, False, [DOWN]))
    half_in(-1, 1, 1)
    pool_across(1, -1)
    half_in(1, 0, 3)
    pool_across(2, 1)
    got(columns(-1, 1 - c), pds.at[1])
    unpack((y + 3) % 4, 0)
    got(columns(1, 1 - c), pds.at[2])
    unpack((y + 1) % 4, 0)
    half_in(2, 0, 4)
    half_in(2, 1, 5)
    pool_across(3, 2)
    gup.run((0, 2, True, []))
    got(columns(2, 1 - c), pds.at[3])
    unpack((y + 2) % 4, 0)

    scale = lax.rsqrt(jnp.sum(acc[...], axis=1, keepdims=True) * (1.0 / 2048) + EPS)
    acc[...] = jnp.zeros_like(acc)
    position = iota((LEN, 512), 0) + 1

    def mix(g, carry):
        divisor = jnp.minimum(position, lax.shift_left(2, g)).astype(f32)
        normed = (xg[g].astype(f32) * scale * gains[g, 0:1, :]).astype(bf16)
        pooled = []
        for s in range(TOK // LEN):
            part = normed[LEN * s : LEN * s + LEN]
            window = jnp.dot(band[g], part, preferred_element_type=f32)
            pooled.append((window / divisor - part.astype(f32)).astype(bf16))
        mixer = jnp.dot(concat(pooled, 0), wg[g], preferred_element_type=f32) * gains[g, 1:2, :]
        middle = (xg[g].astype(f32) + mixer).astype(bf16)
        xg[g] = middle
        total = acc[...]
        for i in range(4):
            part = middle[:, 128 * i : 128 * i + 128].astype(f32)
            total = total + part * part
        acc[...] = total
        return carry

    lax.fori_loop(0, 4, mix, 0)
    scale = lax.rsqrt(jnp.sum(acc[...], axis=1, keepdims=True) * (1.0 / 2048) + EPS)

    def rescale(g, carry):
        xg[g] = (xg[g].astype(f32) * scale * gains[g, 2:3, :]).astype(bf16)
        return carry

    lax.fori_loop(0, 4, rescale, 0)

    def natural(yy, carry):
        at = pl.ds(pl.multiple_of(yy * 128, 128), 128)
        grouped = concat([xg[g, :, at] for g in range(4)], 1)
        moved = jnp.dot(grouped, unperm[...], preferred_element_type=f32).astype(bf16)
        for i in range(4):
            nf[4 * yy + i] = moved[:, 128 * i : 128 * i + 128]
        return carry

    lax.fori_loop(0, 4, natural, 0)

    SETS = ([(0, 0)] + NEAR, FAR + DIAG, KNIGHT + [(2, 2)])
    CHUNKS = ((0, 256), (256, 256), (512, 192))

    def product(core, which, at, width, offsets):
        js = [at_fs(dx, dz) for dx, dz in offsets]
        left = concat([nf[j] for j in js], 1)
        right = concat([gu[core, j, pl.ds(704 * which + at, width), :] for j in js], 1)
        return lax.dot_general(left, right, (((1,), (1,)), ((), ())), preferred_element_type=f32)

    def gather_up(core, i):
        for which in range(2):
            for at, width in CHUNKS:
                part = product(core, which, at, width, SETS[i])
                if i > 0:
                    part = sums[core, which, :, at : at + width] + part
                sums[core, which, :, at : at + width] = part

    def conv(core, which, at, width):
        v = sums[core, which, :, at : at + width] + product(core, which, at, width, SETS[2])
        v = v.astype(bf16).astype(f32)
        k = taps[core, which, :, at : at + width]
        place = iota((TOK, width), 0) % LEN
        back1 = jnp.where(place >= 1, pltpu.roll(v, 1, 0), 0.0)
        back2 = jnp.where(place >= 2, pltpu.roll(v, 2, 0), 0.0)
        return back2 * k[0:1] + back1 * k[1:2] + v * k[2:3]

    def units(core, t):
        at, width = CHUNKS[t]
        a, b = conv(core, 0, at, width), conv(core, 1, at, width)
        hid[core, :, at : at + width] = (a / (1.0 + jnp.exp(-a)) * b).astype(bf16)

    gather_up(c, 0)
    across_wait(gu, gd, 0)
    gather_up(1 - c, 0)
    gup.run((1, -1, True, []), (-1, -1, True, []), (2, -1, True, []))
    gather_up(c, 1)
    down.run((1, 0, True, [RIGHT, UP]))
    across_wait(gu, gd, 1)
    across_wait(gu, gd, 2)
    gather_up(1 - c, 1)
    gup.run((1, 2, True, []), (2, 2, True, []), (-1, 2, True, []))
    units(c, 0)
    down.run((0, 1, True, [UP]))
    units(c, 1)
    down.run((-1, 0, True, [UP, DOWN]), (1, 0, False, [DOWN]))
    units(c, 2)
    across_wait(gu, gd, 3)
    across_wait(gu, gd, 4)
    units(1 - c, 0)
    down.run((0, -1, True, []))
    units(1 - c, 1)
    down.run((2, 0, True, [UP, DOWN]))
    units(1 - c, 2)
    down.run((1, 1, True, [UP]))

    def pair_of(dz, other):
        cols = x // 2 if other == 0 else 1 - x // 2
        zk = (z + dz + 4) % 4
        return zk * 2 + cols, cols, (zk - y + 4) % 4

    def to_owner(k, h, dy, cols):
        slot, device = (3 - dy) // 2, (fs, at_y(dy, cols))
        remote(pb.at[k, h], rbuf.at[slot, c, h], ssem.at[9], rsem.at[slot, c, h], device).start()

    def hand_far(k, h, cols, role):
        dy = 1 - 2 * h

        @pl.when(role == 2)
        def _():
            for p in PIECES:
                there, sem = relay_in.at[h, cols, p], relsem.at[h, cols, p]
                remote(pb.at[k, h, p], there, ssem.at[9], sem, (fs, at_y(dy, c))).start()

    def hand_near(k, h, cols, role):
        dy = 1 - 2 * h

        @pl.when(role == 3 - 2 * h)
        def _():
            to_owner(k, h, -dy, cols)

        @pl.when((role == 0) & (cols == c))
        def _():
            rbuf[0, c, h] = pb[k, h]

        @pl.when((role == 0) & (cols != c))
        def _():
            remote(pb.at[k, h], rbuf.at[0, c, h], ssem.at[9], rsem.at[0, c, h], partner).start()

    def part_of(core, k):
        block = concat([dn[core, 2 * k], dn[core, 2 * k + 1]], 1)
        return jnp.dot(hid[core], block, preferred_element_type=f32)

    def own_part(dz, other, at):
        k, cols, role = pair_of(dz, other)
        early[at] = part_of(c, k)

    def columns_done(k, cols, role, total):
        for h in range(2):
            for p in PIECES:
                pb[k, h, p] = total[LEN * p : LEN * p + LEN, 128 * h : 128 * h + 128].astype(bf16)
        for h in range(2):
            hand_far(k, h, cols, role)
        for h in range(2):
            hand_near(k, h, cols, role)

    def owner_columns(dz, other):
        k, cols, role = pair_of(dz, other)
        columns_done(k, cols, role, part_of(c, k) + part_of(1 - c, k))

    def owner_rest(dz, other, at):
        k, cols, role = pair_of(dz, other)
        columns_done(k, cols, role, early[at] + part_of(1 - c, k))

    def part_at(core, steps):
        block = concat([dn[core, at_fs(dx, dz)] for dx, dz in steps], 1)
        return jnp.dot(hid[core], block, preferred_element_type=f32)

    def halves_done(steps, total, near=True):
        for i, (dx, dz) in enumerate(steps):
            j = at_fs(dx, dz)
            k, h = j // 2, j % 2
            for p in PIECES:
                part = total[LEN * p : LEN * p + LEN, 128 * i : 128 * i + 128]
                pb[k, h, p] = part.astype(bf16)
            hand_far(k, h, k % 2, (k // 2 - y + 4) % 4)
        if near:
            near_done(steps)

    def near_done(steps):
        for dx, dz in steps:
            j = at_fs(dx, dz)
            k, h = j // 2, j % 2
            hand_near(k, h, k % 2, (k // 2 - y + 4) % 4)

    def owner_halves(steps):
        halves_done(steps, part_at(c, steps) + part_at(1 - c, steps))

    def own_halves(steps, at):
        early[at, :, 0 : 128 * len(steps)] = part_at(c, steps)

    def rest_halves(steps, at, near=True):
        halves_done(steps, early[at, :, 0 : 128 * len(steps)] + part_at(1 - c, steps), near)

    def add_half(k, h):
        cols, role = k % 2, (k // 2 - y + 4) % 4

        @pl.when(role == 1 + 2 * h)
        def _():
            for p in PIECES:
                got(relay_in.at[h, cols, p], relsem.at[h, cols, p])
                total = pb[k, h, p].astype(f32) + relay_in[h, cols, p].astype(f32)
                pb[k, h, p] = total.astype(bf16)
                dy = 1 - 2 * h
                there, sem = rbuf.at[(3 - dy) // 2, c, h, p], rsem.at[(3 - dy) // 2, c, h]
                remote(pb.at[k, h, p], there, ssem.at[9], sem, (fs, at_y(dy, cols))).start()

    def half_added(dx, dz):
        j = at_fs(dx, dz)
        add_half(j // 2, j % 2)

    def owner_added(dz, other):
        k, cols, role = pair_of(dz, other)
        for h in range(2):
            add_half(k, h)

    mate = 1 - 2 * (x % 2)
    across_wait(dn, dd, 0)
    owner_columns(0, 0)
    down.run((0, 2, True, []))
    down.run((-1, 1, True, [UP]))
    across_wait(dn, dd, 1)
    owner_columns(0, 1)
    owner_halves([(0, 2)])
    down.run((1, -1, True, []), (-1, -1, True, []))
    own_part(1, 0, 0)
    own_part(-1, 0, 1)
    own_halves([(-mate, 1), (-mate, -1)], 2)
    across_wait(dn, dd, 2)
    owner_rest(1, 0, 0)
    down.run((2, 1, True, [UP]))
    owner_rest(-1, 0, 1)
    rest_halves([(-mate, 1), (-mate, -1)], 2)
    owner_added(0, 0)
    down.run((2, -1, True, []))
    down.run((1, 2, True, []))
    down.run((-1, 2, True, []))
    own_halves([(mate, 2), (-mate, 2)], 0)
    own_halves([(2, 1), (2, -1)], 1)
    owner_added(0, 1)
    half_added(0, 2)
    across_wait(dn, dd, 3)
    rest_halves([(mate, 2), (-mate, 2)], 0, False)
    rest_halves([(2, 1), (2, -1)], 1)
    near_done([(mate, 2), (-mate, 2)])
    down.run((2, 2, True, []))
    own_halves([(2, 2)], 0)
    across_wait(dn, dd, 4)
    rest_halves([(2, 2)], 0)
    owner_added(1, 0)
    owner_added(-1, 0)
    half_added(-mate, 1)
    half_added(-mate, -1)
    half_added(mate, 2)
    half_added(-mate, 2)
    half_added(2, 1)
    half_added(2, -1)
    half_added(2, 2)

    for slot in (1, 2):
        for core in range(2):
            for h in range(2):
                    got(rbuf.at[slot, core, h], rsem.at[slot, core, h])
    for h in range(2):
        got(rbuf.at[0, 1 - c, h], rsem.at[0, 1 - c, h])
    for core in range(2):
        for h in range(2):
            total = sum(rbuf[slot, core, h].reshape(TOK, 128).astype(f32) for slot in range(3))
            out[TOK * core : TOK * core + TOK, 128 * h : 128 * h + 128] = total.astype(bf16)

    for ref, i in (
        (pw.at[0, 0:15], 0), (gu.at[0, 0:15], 1), (dn.at[0, 0:15], 2), (xs.at[0:3], 3), (sv, 4),
        (gu.at[0], 5), (dn.at[0], 6), (pw.at[0:4], 7), (pw.at[0:3], 8), (pb.at[0:7], 9),
    ):
        got(ref, ssem.at[i])


def body(
    stream, gain_mix, pool_weight, pool_gain, gain_ffn, gate_weight, up_weight, gate_taps, up_taps,
    down_weight,
):
    row = lambda v: v.reshape(1, 2048)
    DMA = pltpu.SemaphoreType.DMA
    return pl.pallas_call(
        kernel,
        name="layer",
        out_shape=jax.ShapeDtypeStruct((512, 256), bf16),
        in_specs=[pl.BlockSpec(memory_space=pltpu.HBM)] * 10,
        out_specs=pl.BlockSpec(memory_space=pltpu.VMEM),
        scratch_shapes=[
            pltpu.VMEM((2, 16, 1408, 128), bf16),
            pltpu.VMEM((2, 16, 704, 128), bf16),
            pltpu.VMEM((8, 16, 64, 128), bf16),
            pltpu.VMEM((4, 2, TOK, 256), bf16),
            pltpu.VMEM((TOK, 256), bf16),
            pltpu.VMEM((4, 32, 64), bf16),
            pltpu.VMEM((3, 1, 2048), f32),
            pltpu.VMEM((2, 3, 1408), f32),
            pltpu.VMEM((2, 2, 3, 704), f32),
            pltpu.VMEM((512, 512), bf16),
            pltpu.VMEM((512, 512), bf16),
            pltpu.VMEM((4, LEN, LEN), bf16),
            pltpu.VMEM((4, 8, 512), f32),
            pltpu.VMEM((4, TOK, 512), bf16),
            pltpu.VMEM((4, 512, 512), bf16),
            pltpu.VMEM((16, TOK, 128), bf16),
            pltpu.VMEM((TOK, 128), f32),
            pltpu.VMEM((2, TOK, 704), bf16),
            pltpu.VMEM((8, 2, 2, LEN, 128), bf16),
            pltpu.VMEM((3, 2, 2, 2, LEN, 128), bf16),
            pltpu.VMEM((2, 2, TOK, 704), f32),
            pltpu.VMEM((2, 2, 2, LEN, 128), bf16),
            pltpu.VMEM((4, TOK, 256), f32),
            DMA((11,)),
            DMA((16,)),
            DMA((16,)),
            DMA((2,)),
            DMA((5,)),
            DMA((5,)),
            DMA((6,)),
            DMA((4,)),
            DMA((2, 3)),
            DMA((1,)),
            DMA((3, 2, 2)),
            DMA((10,)),
            DMA((2, 2, 2)),
            pltpu.SemaphoreType.REGULAR,
        ],
        compiler_params=pltpu.CompilerParams(
            collective_id=0, has_side_effects=True, vmem_limit_bytes=50 * 1024 * 1024
        ),
    )(
        *[pltpu.with_memory_space_constraint(v, pltpu.HBM) for v in (
        stream, row(gain_mix), pool_weight, row(pool_gain), row(gain_ffn), gate_weight.T, up_weight.T,
        gate_taps, up_taps, down_weight)]
    )


def solution(mesh):
    return jax.shard_map(
        body,
        mesh=mesh,
        in_specs=(
            P("fs", "tp"), P(), P(None, "fs", "tp"), P(), P(), P("fs", "tp"), P("fs", "tp"), P(), P(),
            P("tp", "fs"),
        ),
        out_specs=P("fs", "tp"),
        check_vma=False,
    )
```
